32 devices in a mesh: ep: 32 (over z, y, x, core).
Axes of the slice: x: 2, y: 2, z: 4, core: 2. Of those that a mesh axis runs over, the one named last changes fastest.
Arguments:
- tokens: bfloat16 [512, 2048], P('ep'), may hold values from -6 to 6
- recurrent_state: float32 [512, 16, 4096], P('ep'), may hold values from -8 to 8
- first_gain: float32 [2048], replicated, may hold values from 0.1 to 1.9
- w_receptance: bfloat16 [2048, 1024], P('ep'), may hold values from -0.125 to 0.125
- w_key: bfloat16 [2048, 1024], P('ep'), may hold values from -0.125 to 0.125
- w_value: bfloat16 [2048, 1024], P('ep'), may hold values from -0.125 to 0.125
- decay_down: bfloat16 [2048, 64], replicated, may hold values from -0.125 to 0.125
- decay_up: bfloat16 [64, 1024], replicated, may hold values from -0.75 to 0.75
- decay_base: float32 [1024], replicated, may hold values from -4 to 1
- rate_down: bfloat16 [2048, 64], replicated, may hold values from -0.125 to 0.125
- rate_up: bfloat16 [64, 1024], replicated, may hold values from -0.75 to 0.75
- rate_base: float32 [1024], replicated, may hold values from -5 to 5
- key_scale: float32 [1024], replicated, may hold values from 0.25 to 4
- head_gain: float32 [1024], replicated, may hold values from 0.1 to 1.9
- w_output: bfloat16 [1024, 2048], replicated, may hold values from -0.1875 to 0.1875
- second_gain: float32 [2048], replicated, may hold values from 0.1 to 1.9
- shared_gate: bfloat16 [2048, 512], replicated, may hold values from -0.125 to 0.125
- shared_up: bfloat16 [2048, 512], replicated, may hold values from -0.125 to 0.125
- shared_down: bfloat16 [512, 2048], replicated, may hold values from -0.25 to 0.25
- expert_gate: bfloat16 [32, 2048, 512], P('ep'), may hold values from -0.125 to 0.125
- expert_up: bfloat16 [32, 2048, 512], P('ep'), may hold values from -0.125 to 0.125
- expert_down: bfloat16 [32, 512, 2048], P('ep'), may hold values from -0.25 to 0.25
- routes: int32 [512, 4], replicated, may hold values from 0 to 31, all different within a row; in each aligned block of 16 rows (0 to 15, 16 to 31, ...) at most 4 rows name the same one
- route_weights: float32 [512, 4], replicated, may hold values from 0.1 to 1
Outputs:
- new_tokens: bfloat16 [512, 2048], P('ep')
- new_state: float32 [512, 16, 4096], P('ep')
The draws below stay inside these ranges and needn't reach their ends.
Inputs may be any that keep to these rules, and one draw needn't show every extreme that they name: `routes`: each row names 4 different experts. In the rows of one device no expert is named by more than 4 rows, a bound that some block reaches of them.
All inputs are finite; a program needn't handle non-finite values.
Results may differ from the reference program's by a relative error of at most 0.015.
Values may be sent and summed in bfloat16 or wider, within the bound.
A program may use at most 128 MiB of HBM per device.

```python
import math
import jax
import jax.numpy as jnp
import numpy as np
from jax import lax

D = 2048
HEADS = 16
HEAD = 64
DECAY_RANK = 64
RATE_RANK = 64
EXPERT_W = 512
SHARED_W = 512
TOPK = 4
MOST = 4
SEQ_DEV = 16
MIX = 1024
STATE = 4096
EXPERTS = 32
TOKENS = 512
N_EP = 32


def block_levels(key, dims, split, least, largest):
    def one(position, blocks):
        heights = jax.random.uniform(jax.random.fold_in(jax.random.fold_in(key, 6), position), (blocks,), jnp.float32, least / len(split), largest / len(split))
        return jnp.repeat(jnp.exp(heights), dims[position] // blocks).reshape((-1,) + (1,) * (len(dims) - position - 1))

    level = one(*split[0])
    for cut in split[1:]:
        level = level * one(*cut)
    return level


def assign_block(rng, own, number, rows, count, top, most, skew):
    sequence = jax.random.permutation(rng, count)
    heavy_load, common = load_shares(count, rows * top, most, skew, True), load_shares(count, rows * top, most, skew, False)
    places = jnp.arange(count)

    def named(sizes, rotation):
        used = int((sizes > 0).sum())
        fixed = max(1, used // 4)
        shifted = fixed + (places - fixed + rotation * (used - fixed)) % max(1, count - fixed)
        return jnp.zeros((count,), jnp.int32).at[sequence[jnp.where(places < fixed, places, shifted)]].set(jnp.asarray(sizes, jnp.int32))

    sizes = jnp.where(number % 4 == 0, named(heavy_load, number // 4), named(common, number - number // 4 - 1))
    mixed = jax.random.permutation(jax.random.fold_in(own, 3), count)
    donor, sink = mixed[0:count // 2 * 2:2], mixed[1:count // 2 * 2:2]
    slack = jnp.minimum(sizes[donor] - 1, most - sizes[sink]) // 2
    slack = jnp.where((donor == sequence[0]) | (sink == sequence[0]) | (sizes[sink] == 0), 0, jnp.maximum(slack, 0))
    shifted = jax.random.randint(jax.random.fold_in(own, 4), (count // 2,), 0, 1 << 20) % (slack + 1)
    sizes = sizes.at[donor].add(-shifted).at[sink].add(shifted)
    labels = jnp.searchsorted(jnp.cumsum(sizes), jnp.arange(rows * top), side="right").astype(jnp.int32)
    listing = labels.reshape(top, rows).T
    listing = listing[jax.random.permutation(jax.random.fold_in(own, 1), rows)]
    rotation = jax.random.randint(jax.random.fold_in(own, 2), (rows, 1), 0, top)
    return jnp.take_along_axis(listing, (jnp.arange(top)[None, :] + rotation) % top, axis=1)


def load_shares(amount, total, bound, skew, full):
    loads = [(1 << 20) // math.isqrt(rank ** skew) + 1 for rank in range(1, amount + 1)]
    largest = bound if full else min(bound, max(-(-total // amount), total * loads[0] // sum(loads)))
    least = 1 if total - largest >= amount - 1 else 0
    given, surplus = [largest] + [least] * (amount - 1), total - largest - least * (amount - 1)
    while surplus > 0:
        candidates = [i for i in range(1, amount) if given[i] < largest] or [i for i in range(1, amount) if given[i] < bound]
        pool, left = sum([loads[i] for i in candidates]), surplus
        for i in candidates:
            addition = min(bound - given[i], max(1, left * loads[i] // pool), surplus)
            given[i] = given[i] + addition
            surplus = surplus - addition
    return np.array(given)


def bell_draw(own_key, dims, scale, most, split=(), kind=jnp.bfloat16):
    factor_of = block_levels(own_key, dims, split, -0.22, 0.18) if split else 1.0
    values = jax.random.normal(own_key, dims, jnp.float32) * scale * factor_of
    return jnp.minimum(jnp.maximum(values, -most), most).astype(kind)


def setup_inputs(seed: int = 0) -> dict:
    arg_keys = jax.random.split(jax.random.key(seed), 25)
    tokens = bell_draw(arg_keys[0], (TOKENS, D), 1.0, 6.0, ((0, 32),))
    recurrent_state = bell_draw(arg_keys[1], (TOKENS, HEADS, STATE), 2.0, 8.0, ((0, 32),), jnp.float32)
    first_gain = jnp.clip(1.0 + 0.18 * jax.random.normal(arg_keys[2], (D,), jnp.float32), 0.1, 1.9)
    w_receptance = bell_draw(arg_keys[3], (D, MIX), D ** -0.5, 0.125, ((0, 32),))
    w_key = bell_draw(arg_keys[4], (D, MIX), D ** -0.5, 0.125, ((0, 32),))
    w_value = bell_draw(arg_keys[5], (D, MIX), D ** -0.5, 0.125, ((0, 32),))
    decay_down = bell_draw(arg_keys[6], (D, DECAY_RANK), D ** -0.5, 0.125)
    decay_up = bell_draw(arg_keys[7], (DECAY_RANK, MIX), DECAY_RANK ** -0.5, 0.75)
    decay_base = jnp.clip(jax.random.uniform(arg_keys[8], (MIX,), jnp.float32, -4.0, 1.0), -4.0, 1.0)
    rate_down = bell_draw(arg_keys[9], (D, RATE_RANK), D ** -0.5, 0.125)
    rate_up = bell_draw(arg_keys[10], (RATE_RANK, MIX), RATE_RANK ** -0.5, 0.75)
    rate_base = bell_draw(arg_keys[11], (MIX,), 2.0, 5.0, (), jnp.float32)
    key_scale = jnp.clip(jnp.exp(jax.random.uniform(arg_keys[12], (MIX,), jnp.float32, math.log(0.25), math.log(4.0))), 0.25, 4.0)
    head_gain = jnp.clip(1.0 + 0.18 * jax.random.normal(arg_keys[13], (MIX,), jnp.float32), 0.1, 1.9)
    w_output = bell_draw(arg_keys[14], (MIX, D), MIX ** -0.5, 0.1875)
    second_gain = jnp.clip(1.0 + 0.18 * jax.random.normal(arg_keys[15], (D,), jnp.float32), 0.1, 1.9)
    shared_gate = bell_draw(arg_keys[16], (D, SHARED_W), D ** -0.5, 0.125)
    shared_up = bell_draw(arg_keys[17], (D, SHARED_W), D ** -0.5, 0.125)
    shared_down = bell_draw(arg_keys[18], (SHARED_W, D), SHARED_W ** -0.5, 0.25)
    expert_gate = bell_draw(arg_keys[19], (EXPERTS, D, EXPERT_W), D ** -0.5, 0.125, ((0, 32),))
    expert_up = bell_draw(arg_keys[20], (EXPERTS, D, EXPERT_W), D ** -0.5, 0.125, ((0, 32),))
    expert_down = bell_draw(arg_keys[21], (EXPERTS, EXPERT_W, D), EXPERT_W ** -0.5, 0.25, ((0, 32),))
    routes_keys = jax.random.split(jax.random.fold_in(arg_keys[22], 1), TOKENS // SEQ_DEV)
    routes_turns = jax.random.permutation(jax.random.fold_in(arg_keys[22], 3), TOKENS // SEQ_DEV)
    routes = jax.vmap(lambda own, number: assign_block(jax.random.fold_in(arg_keys[22], 2), own, number, SEQ_DEV, EXPERTS, TOPK, MOST, 2))(routes_keys, routes_turns).reshape((TOKENS, TOPK))
    route_weights = jnp.clip(jax.random.uniform(arg_keys[23], (TOKENS, TOPK), jnp.float32, 0.1, 1.0), 0.1, 1.0)
    return {"tokens": tokens, "recurrent_state": recurrent_state, "first_gain": first_gain, "w_receptance": w_receptance, "w_key": w_key, "w_value": w_value, "decay_down": decay_down, "decay_up": decay_up, "decay_base": decay_base, "rate_down": rate_down, "rate_up": rate_up, "rate_base": rate_base, "key_scale": key_scale, "head_gain": head_gain, "w_output": w_output, "second_gain": second_gain, "shared_gate": shared_gate, "shared_up": shared_up, "shared_down": shared_down, "expert_gate": expert_gate, "expert_up": expert_up, "expert_down": expert_down, "routes": routes, "route_weights": route_weights}


NORM_EPS = 1e-06
GROUP_EPS = 0.00064

def rms_scale(inputs, gain):
    widened = inputs.astype(jnp.float32)
    return widened * lax.rsqrt(lax.optimization_barrier(jnp.mean(widened * widened, axis=-1, keepdims=True)) + NORM_EPS) * gain

def gated_units(inputs, gate_weight, up_weight):
    gate_part = jnp.dot(inputs, gate_weight, preferred_element_type=jnp.float32)
    up_part = jnp.dot(inputs, up_weight, preferred_element_type=jnp.float32)
    return (jax.nn.silu(gate_part) * up_part).astype(jnp.bfloat16)

def mix_heads(normed, receptance, key_rows, value_rows, state_old, decay_down, decay_up, decay_base, rate_down, rate_up, rate_base, key_scale, head_gain):
    count_rows = normed.shape[0]
    heads_count = state_old.shape[1]
    decay_low = jnp.tanh(jnp.dot(normed, decay_down, preferred_element_type=jnp.float32)).astype(jnp.bfloat16)
    decay_pre = decay_base + jnp.dot(decay_low, decay_up, preferred_element_type=jnp.float32)
    decay_rate = jnp.exp(-jnp.exp(-jax.nn.softplus(-decay_pre) - 0.5))
    rate_low = jnp.dot(normed, rate_down, preferred_element_type=jnp.float32).astype(jnp.bfloat16)
    learn_rate = jax.nn.sigmoid(rate_base + jnp.dot(rate_low, rate_up, preferred_element_type=jnp.float32))

    def by_head(inputs):
        return inputs.astype(jnp.float32).reshape(count_rows, heads_count, HEAD)
    reader = by_head(receptance)
    key_heads = by_head(key_rows)
    value_heads = by_head(value_rows)
    decay_heads = by_head(decay_rate)
    learn_heads = by_head(learn_rate)
    scaled = key_heads * key_scale.reshape(heads_count, HEAD)
    direction = scaled / jnp.sqrt(lax.optimization_barrier(jnp.sum(scaled * scaled, axis=-1, keepdims=True)) + 1.0)
    state_prev = state_old.reshape(count_rows, heads_count, HEAD, HEAD)
    removed = lax.optimization_barrier(jnp.sum(state_prev * direction[:, :, None, :], axis=-1))
    state_next = state_prev * decay_heads[:, :, None, :] - removed[..., None] * (direction * learn_heads)[:, :, None, :] + value_heads[..., None] * key_heads[:, :, None, :]
    readout = lax.optimization_barrier(jnp.sum(state_next * reader[:, :, None, :], axis=-1))
    centre = lax.optimization_barrier(jnp.mean(readout, axis=-1, keepdims=True))
    spread = lax.optimization_barrier(jnp.mean(jnp.square(readout - centre), axis=-1, keepdims=True))
    normalized = ((readout - centre) * lax.rsqrt(spread + GROUP_EPS)).reshape(count_rows, heads_count * HEAD)
    normalized = normalized * head_gain
    return (normalized.astype(jnp.bfloat16), state_next.reshape(count_rows, heads_count, HEAD * HEAD))

def routed_mix(second, routes, route_weights, expert_gate, expert_up, expert_down):
    span_rows = 64
    count_rows = second.shape[0]
    width = second.shape[1]
    experts_all = expert_gate.shape[0]
    flat_expert = routes.reshape(-1).astype(jnp.int32)
    assigned = flat_expert.shape[0]
    flat_token = jnp.arange(assigned, dtype=jnp.int32) // TOPK
    flat_weight = route_weights.reshape(-1)
    ordering = jnp.argsort(flat_expert, stable=True)
    sorted_expert = flat_expert[ordering]
    counts = lax.optimization_barrier(jnp.sum((flat_expert[None, :] == jnp.arange(experts_all, dtype=jnp.int32)[:, None]).astype(jnp.int32), axis=1)).astype(jnp.int32)
    padded = (counts + span_rows - 1) // span_rows * span_rows
    start_sorted = (jnp.cumsum(counts) - counts).astype(jnp.int32)
    end_padded = jnp.cumsum(padded).astype(jnp.int32)
    start_padded = (end_padded - padded).astype(jnp.int32)
    target = (start_padded[sorted_expert] + (jnp.arange(assigned, dtype=jnp.int32) - start_sorted[sorted_expert])).astype(jnp.int32)
    total_rows = (assigned + experts_all * (span_rows - 1) + span_rows - 1) // span_rows * span_rows
    total_spans = total_rows // span_rows
    row_token = jnp.full((total_rows,), count_rows, jnp.int32).at[target].set(flat_token[ordering])
    row_weight = jnp.zeros((total_rows,), jnp.float32).at[target].set(flat_weight[ordering])
    span_expert = jnp.minimum(jnp.searchsorted(end_padded, jnp.arange(total_spans, dtype=jnp.int32) * span_rows, side='right'), experts_all - 1).astype(jnp.int32)
    table = jnp.concatenate([second, jnp.zeros((1, width), second.dtype)], axis=0)

    def one_span(inputs):
        which, token_ids, weights = inputs
        picked = table[token_ids]
        hidden = gated_units(picked, expert_gate[which], expert_up[which])
        result = jnp.dot(hidden, expert_down[which], preferred_element_type=jnp.float32).astype(jnp.bfloat16)
        return result.astype(jnp.float32) * weights[:, None]
    span_out = lax.map(one_span, (span_expert, row_token.reshape(total_spans, span_rows), row_weight.reshape(total_spans, span_rows)))
    summed = jnp.zeros((count_rows + 1, width), jnp.float32).at[row_token].add(span_out.reshape(total_rows, width))
    return summed[:count_rows]

def reference(tokens, recurrent_state, first_gain, w_receptance, w_key, w_value, decay_down, decay_up, decay_base, rate_down, rate_up, rate_base, key_scale, head_gain, w_output, second_gain, shared_gate, shared_up, shared_down, expert_gate, expert_up, expert_down, routes, route_weights):
    normed = rms_scale(tokens, first_gain).astype(jnp.bfloat16)
    receptance = jnp.dot(normed, w_receptance, preferred_element_type=jnp.float32).astype(jnp.bfloat16)
    key_rows = jnp.dot(normed, w_key, preferred_element_type=jnp.float32).astype(jnp.bfloat16)
    value_rows = jnp.dot(normed, w_value, preferred_element_type=jnp.float32).astype(jnp.bfloat16)

    def per_block(group):
        return mix_heads(group[0], group[1], group[2], group[3], group[4], decay_down, decay_up, decay_base, rate_down, rate_up, rate_base, key_scale, head_gain)
    grouped = (normed.reshape(N_EP, SEQ_DEV, D), receptance.reshape(N_EP, SEQ_DEV, MIX), key_rows.reshape(N_EP, SEQ_DEV, MIX), value_rows.reshape(N_EP, SEQ_DEV, MIX), recurrent_state.reshape(N_EP, SEQ_DEV, HEADS, STATE))
    mixed, new_state = lax.map(per_block, grouped)
    mixed = mixed.reshape(TOKENS, MIX)
    new_state = new_state.reshape(TOKENS, HEADS, STATE)
    residual = (tokens.astype(jnp.float32) + jnp.dot(mixed, w_output, preferred_element_type=jnp.float32)).astype(jnp.bfloat16)
    second = rms_scale(residual, second_gain).astype(jnp.bfloat16)
    shared = jnp.dot(gated_units(second, shared_gate, shared_up), shared_down, preferred_element_type=jnp.float32)
    routed = routed_mix(second, routes, route_weights, expert_gate, expert_up, expert_down)
    new_tokens = (residual.astype(jnp.float32) + shared + routed).astype(jnp.bfloat16)
    return (new_tokens, new_state)
```

```python
import functools

import jax
import jax.numpy as jnp
from jax import lax
from jax.experimental import pallas as pl
from jax.experimental.pallas import tpu as pltpu
from jax.sharding import PartitionSpec as P

HEAD = 64
TOPK = 4
MOST = 4
GROUP = 8
PARTS = 4
SPAN = 256
NORM_EPS = 1e-06
GROUP_EPS = 0.00064
MESH = pl.DeviceIdType.MESH
F32 = jnp.float32
BF16 = jnp.bfloat16
VMEM_BYTES = 60 * 1024 * 1024


def dot(a, b):
    return jnp.dot(a, b, preferred_element_type=F32)


def rms_scale(inputs, gain):
    widened = inputs.astype(F32)
    return (
        widened * lax.rsqrt(jnp.mean(widened * widened, axis=-1, keepdims=True) + NORM_EPS) * gain
    )


def project_kernel(
    devices,
    tokens,
    gain,
    w_r,
    w_k,
    w_v,
    decay_down,
    decay_up,
    decay_base,
    rate_down,
    rate_up,
    rate_base,
    key_scale,
    out,
    stage,
    wbuf,
    nsend,
    xbuf,
    psend,
    precv,
    local_sem,
    wsend_sem,
    wrecv_sem,
    xsend_sem,
    xrecv_sem,
    psend_sem,
    precv_sem,
):
    rows, mix = w_r.shape
    half = mix // 2
    count = tokens.shape[0]
    groups = devices // GROUP
    members = 2 * groups
    depth = tokens.shape[1] // groups
    me = lax.axis_index("ep")
    base = (me // GROUP) * GROUP
    place = me % GROUP
    core = me % 2
    column = place // 2
    member = (me // GROUP) * 2 + core
    chip = me - core
    x_bit = (place // 2) % 2
    y_bit = place // 4
    x_chip = chip + 2 - 4 * x_bit
    y_chip = chip + 4 - 8 * y_bit
    diag_chip = x_chip + 4 - 8 * y_bit
    partner = chip + 1 - core

    def peer_of(offset):
        which = (member + offset) % members
        return which, (which // 2) * GROUP + column * 2 + which % 2

    local = []
    weights = (w_r, w_k, w_v)
    for number, weight in enumerate(weights):
        for side in range(2):
            local.append(
                pltpu.make_async_copy(
                    weight.at[:, pl.ds(side * half, half)],
                    stage.at[number, side],
                    local_sem.at[number * 2 + side],
                )
            )
    for copy in local:
        copy.start()

    barrier = pltpu.get_barrier_semaphore()
    greet = [partner, x_chip, x_chip + 1, y_chip, y_chip + 1]
    greet = greet + [peer_of(offset)[1] for offset in range(1, members)]
    for peer in greet:
        pl.semaphore_signal(barrier, inc=1, device_id=(peer,), device_id_type=MESH)

    normed = rms_scale(tokens[...], gain[...]).astype(BF16)
    for number in range(groups):
        nsend[number] = normed[:, number * depth : (number + 1) * depth]
    for copy in local:
        copy.wait()
    pl.semaphore_wait(barrier, len(greet))

    def slot(number, device):
        return wbuf.at[number, pl.ds(pl.multiple_of((device - base) * rows, rows), rows), :]

    def weight_copy(number, source, landing, send, receive, target):
        return pltpu.make_async_remote_copy(
            src_ref=source,
            dst_ref=slot(number, landing),
            send_sem=wsend_sem.at[number * 7 + send],
            recv_sem=wrecv_sem.at[number * 7 + receive],
            device_id=(target,),
            device_id_type=MESH,
        )

    sends = []

    def launch(copy):
        copy.start()
        sends.append(copy)

    def direct(number):
        for side in range(2):
            source = stage.at[number, side]
            launch(weight_copy(number, source, me, 1 + side, 1 + core, x_chip + side))
            launch(weight_copy(number, source, me, 3 + side, 3 + core, y_chip + side))
        launch(weight_copy(number, stage.at[number, 1 - core], me, 0, 0, partner))

    def arrived(number, source, receive):
        weight_copy(number, stage.at[0, 0], source, 0, receive, partner).wait_recv()

    def relay(number):
        arrived(number, y_chip, 3)
        launch(weight_copy(number, slot(number, y_chip), y_chip, 5, 5, x_chip + core))
        arrived(number, x_chip + 1, 2)
        launch(weight_copy(number, slot(number, x_chip + 1), x_chip + 1, 6, 6, y_chip + core))

    direct(0)
    for offset in range(1, members):
        which, device = peer_of(offset)
        launch(
            pltpu.make_async_remote_copy(
                src_ref=nsend.at[which // 2],
                dst_ref=xbuf.at[member],
                send_sem=xsend_sem.at[offset],
                recv_sem=xrecv_sem.at[offset],
                device_id=(device,),
                device_id_type=MESH,
            )
        )
    direct(1)

    for number in range(3):
        own = stage[number, core]
        wbuf[number, pl.ds(pl.multiple_of(place * rows, rows), rows), :] = own
    xbuf[member] = nsend[me // GROUP]
    relay(0)
    direct(2)

    def put(number, values, first):
        for head in range(values.shape[1] // HEAD):
            out[number, :, first + head, :] = values[:, head * HEAD : (head + 1) * HEAD]

    heads = mix // HEAD
    flip = (((1,), (1,)), ((), ()))

    def down(matrix):
        return lax.dot_general(normed, matrix, flip, preferred_element_type=F32)

    decay_low = jnp.tanh(down(decay_down[...])).astype(BF16)
    decay_pre = decay_base[...] + dot(decay_low, decay_up[...])
    put(3, jnp.exp(-jnp.exp(-jax.nn.softplus(-decay_pre) - 0.5)), 0)
    rate_low = down(rate_down[...]).astype(BF16)
    put(4, jax.nn.sigmoid(rate_base[...] + dot(rate_low, rate_up[...])), 0)

    for offset in range(1, members):
        source = (member + members - offset) % members
        pltpu.make_async_remote_copy(
            src_ref=nsend.at[0],
            dst_ref=xbuf.at[source],
            send_sem=xsend_sem.at[offset],
            recv_sem=xrecv_sem.at[offset],
            device_id=(partner,),
            device_id_type=MESH,
        ).wait_recv()
    stacked = xbuf[...].reshape(members * count, depth)

    def part_copy(number, source, landing, offset, target):
        return pltpu.make_async_remote_copy(
            src_ref=psend.at[number, source],
            dst_ref=precv.at[number, landing],
            send_sem=psend_sem.at[number * members + offset],
            recv_sem=precv_sem.at[number * members + offset],
            device_id=(target,),
            device_id_type=MESH,
        )

    def multiply(number):
        arrived(number, partner, 0)
        arrived(number, x_chip, 1)
        arrived(number, y_chip + 1, 4)
        arrived(number, diag_chip, 5)
        arrived(number, diag_chip + 1, 6)
        part = dot(stacked, wbuf[number]).astype(BF16)
        psend[number] = part.reshape(members, count, half)
        for offset in range(1, members):
            which, device = peer_of(offset)
            launch(part_copy(number, which, member, offset, device))
        precv[number, member] = psend[number, member]

    def finish(number):
        for offset in range(1, members):
            source = (member + members - offset) % members
            part_copy(number, 0, source, offset, partner).wait_recv()
        for side in range(2):
            total = precv[number, side].astype(F32)
            for which in range(1, groups):
                total = total + precv[number, which * 2 + side].astype(F32)
            total = total.astype(BF16).astype(F32)
            put(number, total, side * (heads // 2))
            if number == 1:
                scale = key_scale[:, side * half : (side + 1) * half]
                put(5, total * scale, side * (heads // 2))

    relay(1)
    multiply(0)
    relay(2)
    multiply(1)
    finish(0)
    multiply(2)
    finish(1)
    finish(2)
    for copy in sends:
        copy.wait_send()


def project(devices, tokens, gain, w_r, w_k, w_v, dd, du, db, rd, ru, rb, scale):
    count, width = tokens.shape
    rows, mix = w_r.shape
    groups = devices // GROUP
    members = 2 * groups
    half = mix // 2
    vmem = pl.BlockSpec(memory_space=pltpu.VMEM)
    hbm = pl.BlockSpec(memory_space=pl.ANY)
    dma = pltpu.SemaphoreType.DMA
    return pl.pallas_call(
        functools.partial(project_kernel, devices),
        out_shape=jax.ShapeDtypeStruct((6, count, mix // HEAD, HEAD), F32),
        in_specs=[vmem, vmem, hbm, hbm, hbm] + [vmem] * 7,
        out_specs=vmem,
        scratch_shapes=[
            pltpu.VMEM((3, 2, rows, half), BF16),
            pltpu.VMEM((3, GROUP * rows, half), BF16),
            pltpu.VMEM((groups, count, width // groups), BF16),
            pltpu.VMEM((members, count, width // groups), BF16),
            pltpu.VMEM((3, members, count, half), BF16),
            pltpu.VMEM((3, members, count, half), BF16),
            dma((6,)),
            dma((21,)),
            dma((21,)),
            dma((members,)),
            dma((members,)),
            dma((3 * members,)),
            dma((3 * members,)),
        ],
        compiler_params=pltpu.CompilerParams(
            collective_id=0, has_side_effects=True, vmem_limit_bytes=VMEM_BYTES
        ),
        name="project",
    )(tokens, gain, w_r, w_k, w_v, dd, du, db, rd, ru, rb, scale)


def split_sum(values, ones):
    high = values.astype(BF16)
    low = (values - high.astype(F32)).astype(BF16)
    return dot(high, ones) + dot(low, ones)


def mixer_kernel(
    vectors_in,
    state_in,
    head_gain,
    tokens,
    w_output,
    second_gain,
    new_state,
    residual,
    second,
    vectors,
    state,
    fresh_out,
    wbuf,
    mixed,
    work,
    sums,
    vec_sem,
    in_sem,
    out_sem,
    w_sem,
):
    _, count, heads, _ = vectors.shape
    entries = state.shape[2]
    steps = in_sem.shape[0]
    per_step = count // steps
    span = SPAN
    tiles = entries // span
    copies = span // HEAD

    def rows_of(step):
        return pl.ds(step * per_step, per_step)

    def state_load(step):
        return pltpu.make_async_copy(
            state_in.at[rows_of(step)], state.at[rows_of(step)], in_sem.at[step]
        )

    vector_load = pltpu.make_async_copy(vectors_in, vectors, vec_sem)
    weight_load = pltpu.make_async_copy(w_output, wbuf, w_sem)
    vector_load.start()
    for step in range(steps):
        state_load(step).start()
    weight_load.start()

    row = lax.broadcasted_iota(jnp.int32, (span, span), 0)
    col = lax.broadcasted_iota(jnp.int32, (span, span), 1)
    ones = (row // HEAD == col // HEAD).astype(F32).astype(BF16)
    lane = lax.broadcasted_iota(jnp.int32, (heads, span), 1)

    def widen(inputs):
        return jnp.concatenate([inputs] * copies, axis=1)

    vector_load.wait()

    def one_step(step, carry):
        state_load(step).wait()
        size = tiles * heads
        kept = []
        for place in range(per_step):
            number = step * per_step + place
            reader, keys, values, decay, learn, scaled = [vectors[w, number] for w in range(6)]
            direction = scaled / jnp.sqrt(jnp.sum(scaled * scaled, axis=-1, keepdims=True) + 1.0)
            learned = direction * learn
            wide_direction = widen(direction)
            wide_values = widen(values)
            wide_reader = widen(reader * decay)
            base = place * 3 * size
            for i in range(tiles):
                block = state[number, :, i * span : (i + 1) * span]
                pick = lane % HEAD == i * copies + lane // HEAD
                part = slice(base + i * heads, base + (i + 1) * heads)
                work[part] = (block * wide_direction).astype(BF16)
                part = slice(base + size + i * heads, base + size + (i + 1) * heads)
                work[part] = jnp.where(pick, wide_values, 0.0).astype(BF16)
                product = block * wide_reader
                high = product.astype(BF16)
                part = slice(base + 2 * size + i * heads, base + 2 * size + (i + 1) * heads)
                work[part] = high
            along_learned = jnp.sum(learned * reader, axis=-1, keepdims=True)
            along_keys = jnp.sum(keys * reader, axis=-1, keepdims=True)
            kept.append(
                (number, base, widen(decay), widen(learned), widen(keys))
                + (along_learned, along_keys, values)
            )
        sums[...] = dot(work[...], ones)
        for number, base, wide_decay, wide_learn, wide_keys, along_learned, along_keys, values in kept:
            picked_removed = jnp.zeros((heads, span), F32)
            picked_read = jnp.zeros((heads, span), F32)
            for i in range(tiles):
                block = state[number, :, i * span : (i + 1) * span]
                pick = lane % HEAD == i * copies + lane // HEAD

                def summed(which):
                    first = base + which * size + i * heads
                    return sums[first : first + heads]

                removed = summed(0)
                fresh_out[number, :, i * span : (i + 1) * span] = (
                    block * wide_decay - removed * wide_learn + summed(1) * wide_keys
                )
                picked_removed = jnp.where(pick, removed, picked_removed)
                picked_read = jnp.where(pick, summed(2), picked_read)
            picked = picked_read - picked_removed * along_learned
            readout = values * along_keys
            for i in range(copies):
                readout = readout + picked[:, i * HEAD : (i + 1) * HEAD]
            centre = jnp.mean(readout, axis=-1, keepdims=True)
            spread = jnp.mean(jnp.square(readout - centre), axis=-1, keepdims=True)
            mixed[number] = (readout - centre) * lax.rsqrt(spread + GROUP_EPS)
        pltpu.make_async_copy(
            fresh_out.at[rows_of(step)], new_state.at[rows_of(step)], out_sem
        ).start()
        return carry

    lax.fori_loop(0, steps, one_step, 0)

    channels = heads * HEAD
    flat = mixed[...].reshape(count * heads, HEAD)
    source = lax.broadcasted_iota(jnp.int32, (HEAD, channels), 0)
    target = lax.broadcasted_iota(jnp.int32, (HEAD, channels), 1)
    tiled = split_sum(flat, (target % HEAD == source).astype(F32).astype(BF16))
    head = lax.broadcasted_iota(jnp.int32, (count * heads, channels), 0) % heads
    channel = lax.broadcasted_iota(jnp.int32, (count * heads, channels), 1) // HEAD
    kept = (jnp.where(head == channel, tiled, 0.0) * head_gain[...]).astype(BF16)
    owner = lax.broadcasted_iota(jnp.int32, (count, count * heads), 1) // heads
    token = lax.broadcasted_iota(jnp.int32, (count, count * heads), 0)
    rows = dot((owner == token).astype(F32).astype(BF16), kept).astype(BF16)
    weight_load.wait()
    after = (tokens[...].astype(F32) + dot(rows, wbuf[...])).astype(BF16)
    residual[...] = after
    second[...] = rms_scale(after, second_gain[...]).astype(BF16)
    pltpu.make_async_copy(fresh_out, new_state, out_sem).wait()


def mixer(vectors, state, head_gain, tokens, w_output, second_gain):
    _, count, heads, _ = vectors.shape
    width = tokens.shape[1]
    per_step = 8 if count % 8 == 0 else 1
    steps = count // per_step
    rows = per_step * 3 * state.shape[1] * (state.shape[2] // SPAN)
    vmem = pl.BlockSpec(memory_space=pltpu.VMEM)
    hbm = pl.BlockSpec(memory_space=pl.ANY)
    dma = pltpu.SemaphoreType.DMA
    return pl.pallas_call(
        mixer_kernel,
        out_shape=[
            jax.ShapeDtypeStruct(state.shape, F32),
            jax.ShapeDtypeStruct((count, width), BF16),
            jax.ShapeDtypeStruct((count, width), BF16),
        ],
        in_specs=[hbm, hbm, vmem, vmem, hbm, vmem],
        out_specs=[hbm, vmem, vmem],
        scratch_shapes=[
            pltpu.VMEM(vectors.shape, F32),
            pltpu.VMEM(state.shape, F32),
            pltpu.VMEM(state.shape, F32),
            pltpu.VMEM(w_output.shape, BF16),
            pltpu.VMEM((count, heads, HEAD), F32),
            pltpu.VMEM((rows, SPAN), BF16),
            pltpu.VMEM((rows, SPAN), F32),
            dma,
            dma((steps,)),
            dma,
            dma,
        ],
        compiler_params=pltpu.CompilerParams(vmem_limit_bytes=VMEM_BYTES),
        name="mixer",
    )(vectors, state, head_gain, tokens, w_output, second_gain)


def onehot(flags):
    return flags.astype(F32).astype(BF16)


def onehot_values(values):
    return values.astype(F32).astype(BF16)


def thirds(values):
    first = values.astype(BF16)
    rest = values - first.astype(F32)
    middle = rest.astype(BF16)
    return first, middle, (rest - middle.astype(F32)).astype(BF16)


def experts_kernel(
    devices,
    second,
    residual,
    routes,
    route_weights,
    shared_gate,
    shared_up,
    shared_down,
    expert_gate,
    expert_up,
    expert_down,
    out,
    sg,
    su,
    sd,
    eg,
    eu,
    ed,
    sbuf,
    rbuf,
    pbuf,
    abuf,
    xfull,
    local_sem,
    osend_sem,
    orecv_sem,
    bsend_sem,
    brecv_sem,
):
    count, width = second.shape
    part = width // PARTS
    block = PARTS * MOST
    total = devices * block
    tall = PARTS * count
    me = lax.axis_index("ep")
    barrier = pltpu.get_barrier_semaphore()

    def greet(offset, carry):
        pl.semaphore_signal(
            barrier, inc=1, device_id=((me + offset) % devices,), device_id_type=MESH
        )
        return carry

    lax.fori_loop(1, devices, greet, 0)
    loads = [
        pltpu.make_async_copy(source, target, local_sem.at[number])
        for number, (source, target) in enumerate(
            (
                (shared_gate, sg),
                (shared_up, su),
                (expert_gate.at[0], eg),
                (expert_up.at[0], eu),
                (shared_down, sd),
                (expert_down.at[0], ed),
            )
        )
    ]
    for load in loads:
        load.start()

    rows = second[...]
    lines = lax.broadcasted_iota(jnp.int32, (routes.shape[1], PARTS * count), 0)
    lanes = lax.broadcasted_iota(jnp.int32, (routes.shape[1], PARTS * count), 1)
    pick = onehot(lines == me * count + lanes % count)
    routes_wide = dot(onehot_values(routes[...]), pick)
    stacked = jnp.concatenate([rows[:, q * part : (q + 1) * part] for q in range(PARTS)], 0)
    line = lax.broadcasted_iota(jnp.int32, (total, tall), 0)
    lane = lax.broadcasted_iota(jnp.int32, (total, tall), 1)
    named = line < 0
    for j in range(TOPK):
        named = named | (routes_wide[j : j + 1, :] == (line // block).astype(F32))
    up_row = lax.broadcasted_iota(jnp.int32, (tall, tall), 0)
    up_col = lax.broadcasted_iota(jnp.int32, (tall, tall), 1)
    same = up_row // count == up_col // count
    before = dot(onehot(named), onehot(same & (up_row < up_col)))
    fits = (before == (line % MOST).astype(F32)) & (lane // count == (line % block) // MOST)
    outgoing = dot(onehot(named & fits), stacked).astype(BF16)
    sbuf[...] = outgoing.reshape(devices, block, part)
    pl.semaphore_wait(barrier, devices - 1)

    def exchange(source_ref, target_ref, send, receive, offset, landing):
        peer = (me + offset) % devices
        return pltpu.make_async_remote_copy(
            src_ref=source_ref.at[peer],
            dst_ref=target_ref.at[landing],
            send_sem=send.at[offset],
            recv_sem=receive.at[offset],
            device_id=(peer,),
            device_id_type=MESH,
        )

    def start_all(source_ref, target_ref, send, receive):
        def one(turn, carry):
            offset = devices // 2 + (1 - 2 * (turn % 2)) * ((turn + 1) // 2)
            exchange(source_ref, target_ref, send, receive, offset, me).start()
            return carry

        lax.fori_loop(0, devices - 1, one, 0)

    def receive_all(source_ref, target_ref, send, receive):
        def one(offset, carry):
            origin = (me + devices - offset) % devices
            exchange(source_ref, target_ref, send, receive, offset, origin).wait_recv()
            return carry

        lax.fori_loop(1, devices, one, 0)

    def sent_all(source_ref, target_ref, send, receive):
        def one(offset, carry):
            exchange(source_ref, target_ref, send, receive, offset, me).wait_send()
            return carry

        lax.fori_loop(1, devices, one, 0)

    there = (sbuf, rbuf, osend_sem, orecv_sem)
    back = (pbuf, abuf, bsend_sem, brecv_sem)
    start_all(*there)
    rbuf[me] = sbuf[me]

    def gated(inputs, gate_ref, up_ref):
        gate_part = dot(inputs, gate_ref[...])
        up_part = dot(inputs, up_ref[...])
        return (jax.nn.silu(gate_part) * up_part).astype(BF16)

    loads[0].wait()
    loads[1].wait()
    shared_hidden = gated(rows, sg, su)
    loads[4].wait()
    shared = dot(shared_hidden, sd[...])

    across = lax.broadcasted_iota(jnp.int32, (tall, total), 1)
    down = lax.broadcasted_iota(jnp.int32, (tall, total), 0)
    named_t = across < 0
    turned = (((1,), (1,)), ((), ()))
    lines_t = lax.broadcasted_iota(jnp.int32, (tall, routes.shape[1]), 1)
    lanes_t = lax.broadcasted_iota(jnp.int32, (tall, routes.shape[1]), 0)
    pick_t = onehot(lines_t == me * count + lanes_t % count)

    def picked(values):
        return lax.dot_general(pick_t, values, turned, preferred_element_type=F32)

    routes_tall = picked(onehot_values(routes[...]))
    weights_tall = sum(picked(piece) for piece in thirds(route_weights[...]))
    weight_t = jnp.zeros((tall, total), F32)
    for j in range(TOPK):
        hit = routes_tall[:, j : j + 1] == (across // block).astype(F32)
        named_t = named_t | hit
        weight_t = weight_t + jnp.where(hit, weights_tall[:, j : j + 1], 0.0)
    before_t = dot(onehot(same & (up_col < up_row)), onehot(named_t))
    fits_t = (before_t == (across % MOST).astype(F32)) & (
        down // count == (across % block) // MOST
    )
    weight_t = jnp.where(fits_t, weight_t, 0.0)
    first, middle, last = thirds(weight_t)

    slots = devices * MOST
    narrow = lax.broadcasted_iota(jnp.int32, (slots, total), 0)
    broad = lax.broadcasted_iota(jnp.int32, (slots, total), 1)
    tall_row = lax.broadcasted_iota(jnp.int32, (total, slots), 0)
    tall_col = lax.broadcasted_iota(jnp.int32, (total, slots), 1)
    takes = []
    gives = []
    for q in range(PARTS):
        takes.append(onehot(broad == narrow // MOST * block + q * MOST + narrow % MOST))
        gives.append(onehot(tall_row == tall_col // MOST * block + q * MOST + tall_col % MOST))

    receive_all(*there)
    received = rbuf[...].reshape(total, part)
    for q in range(PARTS):
        xfull[:, q * part : (q + 1) * part] = dot(takes[q], received).astype(BF16)
    loads[2].wait()
    loads[3].wait()
    hidden = gated(xfull[...], eg, eu)
    loads[5].wait()
    produced = jnp.zeros((total, part), F32)
    for q in range(PARTS):
        result = dot(hidden, ed[:, q * part : (q + 1) * part]).astype(BF16)
        produced = produced + dot(gives[q], result)
    pbuf[...] = produced.astype(BF16).reshape(devices, block, part)
    start_all(*back)
    abuf[me] = pbuf[me]
    receive_all(*back)
    answers = abuf[...].reshape(total, part)
    routed = dot(first, answers) + dot(middle, answers) + dot(last, answers)
    kept = residual[...].astype(F32) + shared
    for q in range(PARTS):
        cut = slice(q * part, (q + 1) * part)
        out[:, cut] = (kept[:, cut] + routed[q * count : (q + 1) * count]).astype(BF16)
    sent_all(*there)
    sent_all(*back)


def experts(devices, second, residual, routes, weights, *matrices):
    count, width = second.shape
    vmem = pl.BlockSpec(memory_space=pltpu.VMEM)
    hbm = pl.BlockSpec(memory_space=pl.ANY)
    dma = pltpu.SemaphoreType.DMA
    exchange = pltpu.VMEM((devices, PARTS * MOST, width // PARTS), BF16)
    return pl.pallas_call(
        functools.partial(experts_kernel, devices),
        out_shape=jax.ShapeDtypeStruct((count, width), BF16),
        in_specs=[vmem] * 4 + [hbm] * 6,
        out_specs=vmem,
        scratch_shapes=[pltpu.VMEM(m.shape[-2:], BF16) for m in matrices]
        + [exchange] * 4
        + [
            pltpu.VMEM((devices * MOST, width), BF16),
            dma((6,)),
            dma((devices,)),
            dma((devices,)),
            dma((devices,)),
            dma((devices,)),
        ],
        compiler_params=pltpu.CompilerParams(
            collective_id=1, has_side_effects=True, vmem_limit_bytes=VMEM_BYTES
        ),
        name="experts",
    )(second, residual, routes, weights, *matrices)


def per_device(
    tokens,
    recurrent_state,
    first_gain,
    w_receptance,
    w_key,
    w_value,
    decay_down,
    decay_up,
    decay_base,
    rate_down,
    rate_up,
    rate_base,
    key_scale,
    head_gain,
    w_output,
    second_gain,
    shared_gate,
    shared_up,
    shared_down,
    expert_gate,
    expert_up,
    expert_down,
    routes,
    route_weights,
):
    devices = lax.axis_size("ep")
    vectors = project(
        devices,
        tokens,
        first_gain[None, :],
        w_receptance,
        w_key,
        w_value,
        decay_down.T,
        decay_up,
        decay_base[None, :],
        rate_down.T,
        rate_up,
        rate_base[None, :],
        key_scale[None, :],
    )
    new_state, residual, second = mixer(
        vectors,
        recurrent_state,
        head_gain[None, :],
        tokens,
        w_output,
        second_gain[None, :],
    )
    new_tokens = experts(
        devices,
        second,
        residual,
        routes.T,
        route_weights.T,
        shared_gate,
        shared_up,
        shared_down,
        expert_gate,
        expert_up,
        expert_down,
    )
    return (new_tokens, new_state)


def solution(mesh):
    in_specs = (
        P("ep", None),
        P("ep", None, None),
        P(),
        P("ep", None),
        P("ep", None),
        P("ep", None),
        P(),
        P(),
        P(),
        P(),
        P(),
        P(),
        P(),
        P(),
        P(),
        P(),
        P(),
        P(),
        P(),
        P("ep", None, None),
        P("ep", None, None),
        P("ep", None, None),
        P(),
        P(),
    )
    out_specs = (P("ep", None), P("ep", None, None))
    return jax.shard_map(
        per_device, mesh=mesh, in_specs=in_specs, out_specs=out_specs, check_vma=False
    )
```

```python
import functools

import jax
import jax.numpy as jnp
from jax import lax
from jax.experimental import pallas as pl
from jax.experimental.pallas import tpu as pltpu
from jax.sharding import PartitionSpec as P

HEAD = 64
TOPK = 4
MOST = 4
GROUP = 8
PARTS = 4
SPAN = 256
SPLIT = 2
NORM_EPS = 1e-06
GROUP_EPS = 0.00064
MESH = pl.DeviceIdType.MESH
F32 = jnp.float32
BF16 = jnp.bfloat16
VMEM_BYTES = 60 * 1024 * 1024


def dot(a, b):
    return jnp.dot(a, b, preferred_element_type=F32)


def rms_scale(inputs, gain):
    widened = inputs.astype(F32)
    return (
        widened * lax.rsqrt(jnp.mean(widened * widened, axis=-1, keepdims=True) + NORM_EPS) * gain
    )


def project_kernel(
    devices,
    tokens_in,
    gain_in,
    decay_down_in,
    decay_up_in,
    decay_base_in,
    rate_down_in,
    rate_up_in,
    rate_base_in,
    key_scale_in,
    w_r,
    w_k,
    w_v,
    out,
    tokens,
    gain,
    decay_down,
    decay_up,
    decay_base,
    rate_down,
    rate_up,
    rate_base,
    key_scale,
    stage,
    wbuf,
    nsend,
    xbuf,
    psend,
    precv,
    small_sem,
    local_sem,
    wsend_sem,
    wrecv_sem,
    xsend_sem,
    xrecv_sem,
    psend_sem,
    precv_sem,
):
    rows, mix = w_r.shape
    half = mix // 2
    piece = half // SPLIT
    pieces = 3 * SPLIT
    count = tokens.shape[0]
    groups = devices // GROUP
    members = 2 * groups
    depth = tokens.shape[1] // groups
    me = lax.axis_index("ep")
    base = (me // GROUP) * GROUP
    place = me % GROUP
    core = me % 2
    column = place // 2
    member = (me // GROUP) * 2 + core
    chip = me - core
    x_bit = (place // 2) % 2
    y_bit = place // 4
    x_chip = chip + 2 - 4 * x_bit
    y_chip = chip + 4 - 8 * y_bit
    diag_chip = x_chip + 4 - 8 * y_bit
    partner = chip + 1 - core

    def peer_of(offset):
        which = (member + offset) % members
        return which, (which // 2) * GROUP + column * 2 + which % 2

    barrier = pltpu.get_barrier_semaphore()
    greet = [partner, x_chip, x_chip + 1, y_chip, y_chip + 1]
    greet = greet + [peer_of(offset)[1] for offset in range(1, members)]
    for peer in greet:
        pl.semaphore_signal(barrier, inc=1, device_id=(peer,), device_id_type=MESH)

    smalls = [
        pltpu.make_async_copy(source, target, small_sem.at[number])
        for number, (source, target) in enumerate(
            (
                (tokens_in, tokens),
                (gain_in, gain),
                (decay_down_in, decay_down),
                (decay_up_in, decay_up),
                (decay_base_in, decay_base),
                (rate_down_in, rate_down),
                (rate_up_in, rate_up),
                (rate_base_in, rate_base),
                (key_scale_in, key_scale),
            )
        )
    ]
    for small in smalls[:2]:
        small.start()
    for number, weight in enumerate((w_r, w_k, w_v)):
        for sub in range(SPLIT):
            for side in range(2):
                pltpu.make_async_copy(
                    weight.at[:, pl.ds(side * half + sub * piece, piece)],
                    stage.at[number * SPLIT + sub, side],
                    local_sem.at[number],
                ).start()
    for small in smalls[2:]:
        small.start()

    def loaded(number):
        span = stage.at[pl.ds(number * SPLIT, SPLIT)]
        pltpu.make_async_copy(span, span, local_sem.at[number]).wait()

    for small in smalls[:2]:
        small.wait()
    normed = rms_scale(tokens[...], gain[...]).astype(BF16)
    for number in range(groups):
        nsend[number] = normed[:, number * depth : (number + 1) * depth]
    loaded(0)
    pl.semaphore_wait(barrier, len(greet))

    def slot(number, device):
        return wbuf.at[number, pl.ds(pl.multiple_of((device - base) * rows, rows), rows), :]

    def remote(source, target, send, receive, device):
        return pltpu.make_async_remote_copy(
            src_ref=source,
            dst_ref=target,
            send_sem=send,
            recv_sem=receive,
            device_id=(device,),
            device_id_type=MESH,
        )

    def weight_copy(number, source, landing, kind, target):
        return remote(
            source, slot(number, landing), wsend_sem, wrecv_sem.at[number * 3 + kind], target
        )

    def direct(number):
        for side in range(2):
            source = stage.at[number, side]
            own_side = 1 - core
            weight_copy(number, source, me, core * 2, x_chip + side).start()
            weight_copy(number, source, me, own_side, y_chip + side).start()
        weight_copy(number, stage.at[number, 1 - core], me, 0, partner).start()

    def arrived(number, source, kind):
        weight_copy(number, stage.at[0, 0], source, kind, partner).wait_recv()

    def relay(number):
        arrived(number, y_chip, 1)
        weight_copy(number, slot(number, y_chip), y_chip, 0, x_chip + core).start()
        arrived(number, x_chip + 1, 2)
        weight_copy(number, slot(number, x_chip + 1), x_chip + 1, 0, y_chip + core).start()

    def rest(number):
        span = wbuf.at[number, pl.ds(0, 5 * rows), :]
        remote(span, span, wsend_sem, wrecv_sem.at[number * 3], partner).wait_recv()

    def own(number):
        mine = stage[number, core]
        wbuf[number, pl.ds(pl.multiple_of(place * rows, rows), rows), :] = mine

    direct(0)
    for offset in range(1, members):
        which, device = peer_of(offset)
        remote(nsend.at[which // 2], xbuf.at[member], xsend_sem, xrecv_sem, device).start()
    direct(1)
    loaded(1)
    direct(2)
    loaded(2)
    for number in range(pieces):
        own(number)
    xbuf[member] = nsend[me // GROUP]
    relay(0)
    direct(3)

    def put(number, values, first):
        for head in range(values.shape[1] // HEAD):
            out[number, :, first + head, :] = values[:, head * HEAD : (head + 1) * HEAD]

    heads = mix // HEAD
    flip = (((1,), (1,)), ((), ()))

    def down(matrix):
        return lax.dot_general(normed, matrix, flip, preferred_element_type=F32)

    for small in smalls[2:]:
        small.wait()
    decay_low = jnp.tanh(down(decay_down[...])).astype(BF16)
    decay_pre = decay_base[...] + dot(decay_low, decay_up[...])
    put(3, jnp.exp(-jnp.exp(-jax.nn.softplus(-decay_pre) - 0.5)), 0)
    relay(1)
    direct(4)
    rate_low = down(rate_down[...]).astype(BF16)
    put(4, jax.nn.sigmoid(rate_base[...] + dot(rate_low, rate_up[...])), 0)
    relay(2)
    direct(5)

    others = pl.ds(0, members - 1)
    remote(xbuf.at[others], xbuf.at[others], xsend_sem, xrecv_sem, partner).wait_recv()
    stacked = xbuf[...].reshape(members * count, depth)

    def multiply(number):
        rest(number)
        part = dot(stacked, wbuf[number]).astype(BF16)
        psend[number] = part.reshape(members, count, piece)
        for offset in range(1, members):
            which, device = peer_of(offset)
            remote(
                psend.at[number, which],
                precv.at[number, member],
                psend_sem,
                precv_sem.at[number],
                device,
            ).start()
        precv[number, member] = psend[number, member]

    def finish(number):
        span = precv.at[number, others]
        remote(span, span, psend_sem, precv_sem.at[number], partner).wait_recv()
        for side in range(2):
            total = precv[number, side].astype(F32)
            for which in range(1, groups):
                total = total + precv[number, which * 2 + side].astype(F32)
            total = total.astype(BF16).astype(F32)
            column = side * half + number % SPLIT * piece
            put(number // SPLIT, total, column // HEAD)
            if number // SPLIT == 1:
                put(5, total * key_scale[:, column : column + piece], column // HEAD)

    multiply(0)
    relay(3)
    multiply(1)
    relay(4)
    multiply(2)
    relay(5)
    finish(0)
    multiply(3)
    finish(1)
    multiply(4)
    finish(2)
    multiply(5)
    finish(3)
    finish(4)
    finish(5)
    span = wbuf.at[:, pl.ds(0, 7 * rows), :]
    remote(span, span, wsend_sem, wrecv_sem.at[0], partner).wait_send()
    remote(xbuf.at[others], xbuf.at[others], xsend_sem, xrecv_sem, partner).wait_send()
    span = psend.at[:, others]
    remote(span, span, psend_sem, precv_sem.at[0], partner).wait_send()


def project(devices, weights, *smalls):
    count, width = smalls[0].shape
    rows, mix = weights[0].shape
    groups = devices // GROUP
    members = 2 * groups
    piece = mix // 2 // SPLIT
    pieces = 3 * SPLIT
    vmem = pl.BlockSpec(memory_space=pltpu.VMEM)
    hbm = pl.BlockSpec(memory_space=pl.ANY)
    dma = pltpu.SemaphoreType.DMA
    return pl.pallas_call(
        functools.partial(project_kernel, devices),
        out_shape=jax.ShapeDtypeStruct((6, count, mix // HEAD, HEAD), F32),
        in_specs=[hbm] * 12,
        out_specs=vmem,
        scratch_shapes=[pltpu.VMEM(array.shape, array.dtype) for array in smalls]
        + [
            pltpu.VMEM((pieces, 2, rows, piece), BF16),
            pltpu.VMEM((pieces, GROUP * rows, piece), BF16),
            pltpu.VMEM((groups, count, width // groups), BF16),
            pltpu.VMEM((members, count, width // groups), BF16),
            pltpu.VMEM((pieces, members, count, piece), BF16),
            pltpu.VMEM((pieces, members, count, piece), BF16),
            dma((9,)),
            dma((3,)),
            dma,
            dma((3 * pieces,)),
            dma,
            dma,
            dma,
            dma((pieces,)),
        ],
        compiler_params=pltpu.CompilerParams(
            collective_id=0, has_side_effects=True, vmem_limit_bytes=VMEM_BYTES
        ),
        name="project",
    )(*smalls, *weights)


def split_sum(values, ones):
    high = values.astype(BF16)
    low = (values - high.astype(F32)).astype(BF16)
    return dot(high, ones) + dot(low, ones)


def mixer_kernel(
    vectors_in,
    state_in,
    head_gain,
    tokens,
    w_output,
    second_gain,
    new_state,
    residual,
    second,
    vectors,
    state,
    fresh_out,
    wbuf,
    mixed,
    work,
    sums,
    vec_sem,
    in_sem,
    out_sem,
    w_sem,
):
    _, count, heads, _ = vectors.shape
    entries = state.shape[2]
    steps = in_sem.shape[0]
    per_step = count // steps
    span = SPAN
    tiles = entries // span
    copies = span // HEAD

    def rows_of(step):
        return pl.ds(step * per_step, per_step)

    def state_load(step):
        return pltpu.make_async_copy(
            state_in.at[rows_of(step)], state.at[rows_of(step)], in_sem.at[step]
        )

    vector_load = pltpu.make_async_copy(vectors_in, vectors, vec_sem)
    weight_load = pltpu.make_async_copy(w_output, wbuf, w_sem)
    vector_load.start()
    for step in range(steps):
        state_load(step).start()
    weight_load.start()

    row = lax.broadcasted_iota(jnp.int32, (span, span), 0)
    col = lax.broadcasted_iota(jnp.int32, (span, span), 1)
    ones = (row // HEAD == col // HEAD).astype(F32).astype(BF16)
    lane = lax.broadcasted_iota(jnp.int32, (heads, span), 1)

    def widen(inputs):
        return jnp.concatenate([inputs] * copies, axis=1)

    vector_load.wait()

    def one_step(step, carry):
        state_load(step).wait()
        size = tiles * heads
        kept = []
        for place in range(per_step):
            number = step * per_step + place
            reader, keys, values, decay, learn, scaled = [vectors[w, number] for w in range(6)]
            direction = scaled / jnp.sqrt(jnp.sum(scaled * scaled, axis=-1, keepdims=True) + 1.0)
            learned = direction * learn
            wide_direction = widen(direction)
            wide_values = widen(values)
            wide_reader = widen(reader * decay)
            base = place * 3 * size
            for i in range(tiles):
                block = state[number, :, i * span : (i + 1) * span]
                pick = lane % HEAD == i * copies + lane // HEAD
                part = slice(base + i * heads, base + (i + 1) * heads)
                work[part] = (block * wide_direction).astype(BF16)
                part = slice(base + size + i * heads, base + size + (i + 1) * heads)
                work[part] = jnp.where(pick, wide_values, 0.0).astype(BF16)
                product = block * wide_reader
                high = product.astype(BF16)
                part = slice(base + 2 * size + i * heads, base + 2 * size + (i + 1) * heads)
                work[part] = high
            along_learned = jnp.sum(learned * reader, axis=-1, keepdims=True)
            along_keys = jnp.sum(keys * reader, axis=-1, keepdims=True)
            kept.append(
                (number, base, widen(decay), widen(learned), widen(keys))
                + (along_learned, along_keys, values)
            )
        sums[...] = dot(work[...], ones)
        for number, base, wide_decay, wide_learn, wide_keys, along_learned, along_keys, values in kept:
            picked_removed = jnp.zeros((heads, span), F32)
            picked_read = jnp.zeros((heads, span), F32)
            for i in range(tiles):
                block = state[number, :, i * span : (i + 1) * span]
                pick = lane % HEAD == i * copies + lane // HEAD

                def summed(which):
                    first = base + which * size + i * heads
                    return sums[first : first + heads]

                removed = summed(0)
                fresh_out[number, :, i * span : (i + 1) * span] = (
                    block * wide_decay - removed * wide_learn + summed(1) * wide_keys
                )
                picked_removed = jnp.where(pick, removed, picked_removed)
                picked_read = jnp.where(pick, summed(2), picked_read)
            picked = picked_read - picked_removed * along_learned
            readout = values * along_keys
            for i in range(copies):
                readout = readout + picked[:, i * HEAD : (i + 1) * HEAD]
            centre = jnp.mean(readout, axis=-1, keepdims=True)
            spread = jnp.mean(jnp.square(readout - centre), axis=-1, keepdims=True)
            mixed[number] = (readout - centre) * lax.rsqrt(spread + GROUP_EPS)
        pltpu.make_async_copy(
            fresh_out.at[rows_of(step)], new_state.at[rows_of(step)], out_sem
        ).start()
        return carry

    lax.fori_loop(0, steps, one_step, 0)

    channels = heads * HEAD
    flat = mixed[...].reshape(count * heads, HEAD)
    source = lax.broadcasted_iota(jnp.int32, (HEAD, channels), 0)
    target = lax.broadcasted_iota(jnp.int32, (HEAD, channels), 1)
    tiled = split_sum(flat, (target % HEAD == source).astype(F32).astype(BF16))
    head = lax.broadcasted_iota(jnp.int32, (count * heads, channels), 0) % heads
    channel = lax.broadcasted_iota(jnp.int32, (count * heads, channels), 1) // HEAD
    kept = (jnp.where(head == channel, tiled, 0.0) * head_gain[...]).astype(BF16)
    owner = lax.broadcasted_iota(jnp.int32, (count, count * heads), 1) // heads
    token = lax.broadcasted_iota(jnp.int32, (count, count * heads), 0)
    rows = dot((owner == token).astype(F32).astype(BF16), kept).astype(BF16)
    weight_load.wait()
    after = (tokens[...].astype(F32) + dot(rows, wbuf[...])).astype(BF16)
    residual[...] = after
    second[...] = rms_scale(after, second_gain[...]).astype(BF16)
    pltpu.make_async_copy(fresh_out, new_state, out_sem).wait()


def mixer(vectors, state, head_gain, tokens, w_output, second_gain):
    _, count, heads, _ = vectors.shape
    width = tokens.shape[1]
    per_step = 8 if count % 8 == 0 else 1
    steps = count // per_step
    rows = per_step * 3 * state.shape[1] * (state.shape[2] // SPAN)
    vmem = pl.BlockSpec(memory_space=pltpu.VMEM)
    hbm = pl.BlockSpec(memory_space=pl.ANY)
    dma = pltpu.SemaphoreType.DMA
    return pl.pallas_call(
        mixer_kernel,
        out_shape=[
            jax.ShapeDtypeStruct(state.shape, F32),
            jax.ShapeDtypeStruct((count, width), BF16),
            jax.ShapeDtypeStruct((count, width), BF16),
        ],
        in_specs=[hbm, hbm, vmem, vmem, hbm, vmem],
        out_specs=[hbm, vmem, vmem],
        scratch_shapes=[
            pltpu.VMEM(vectors.shape, F32),
            pltpu.VMEM(state.shape, F32),
            pltpu.VMEM(state.shape, F32),
            pltpu.VMEM(w_output.shape, BF16),
            pltpu.VMEM((count, heads, HEAD), F32),
            pltpu.VMEM((rows, SPAN), BF16),
            pltpu.VMEM((rows, SPAN), F32),
            dma,
            dma((steps,)),
            dma,
            dma,
        ],
        compiler_params=pltpu.CompilerParams(vmem_limit_bytes=VMEM_BYTES),
        name="mixer",
    )(vectors, state, head_gain, tokens, w_output, second_gain)


def onehot(flags):
    return flags.astype(F32).astype(BF16)


def onehot_values(values):
    return values.astype(F32).astype(BF16)


def thirds(values):
    first = values.astype(BF16)
    rest = values - first.astype(F32)
    middle = rest.astype(BF16)
    return first, middle, (rest - middle.astype(F32)).astype(BF16)


def experts_kernel(
    devices,
    second_in,
    residual_in,
    routes_in,
    route_weights_in,
    shared_gate,
    shared_up,
    shared_down,
    expert_gate,
    expert_up,
    expert_down,
    out,
    second,
    residual,
    routes,
    route_weights,
    sg,
    su,
    sd,
    eg,
    eu,
    ed,
    sbuf,
    rbuf,
    pbuf,
    abuf,
    hops,
    xfull,
    small_sem,
    local_sem,
    send_sem,
    recv_sem,
    hop_send_sem,
    hop_recv_sem,
):
    count, width = second.shape
    part = width // PARTS
    block = PARTS * MOST
    total = devices * block
    tall = PARTS * count
    groups = devices // GROUP
    relayed = 0
    me = lax.axis_index("ep")
    group = me // GROUP
    place = me % GROUP
    barrier = pltpu.get_barrier_semaphore()
    smalls = [
        pltpu.make_async_copy(source, target, small_sem.at[number])
        for number, (source, target) in enumerate(
            (
                (routes_in, routes),
                (second_in, second),
                (route_weights_in, route_weights),
                (residual_in, residual),
            )
        )
    ]
    for small in smalls:
        small.start()

    def peers():
        order = sorted(range(groups), key=lambda g: (-min(g, groups - g), g))
        for far in order:
            base = lax.rem(group + far, groups) * GROUP
            for near in range(GROUP):
                if far or near:
                    yield far, near, base + lax.rem(place + near, GROUP)

    for _, _, peer in peers():
        pl.semaphore_signal(barrier, inc=1, device_id=(peer,), device_id_type=MESH)
    loads = [
        pltpu.make_async_copy(source, target, local_sem.at[number])
        for number, (source, target) in enumerate(
            (
                (shared_gate, sg),
                (shared_up, su),
                (shared_down, sd),
                (expert_gate.at[0], eg),
                (expert_up.at[0], eu),
                (expert_down.at[0], ed),
            )
        )
    ]
    for load in loads:
        load.start()

    smalls[0].wait()
    lines = lax.broadcasted_iota(jnp.int32, (routes.shape[1], PARTS * count), 0)
    lanes = lax.broadcasted_iota(jnp.int32, (routes.shape[1], PARTS * count), 1)
    pick = onehot(lines == me * count + lanes % count)
    routes_wide = dot(onehot_values(routes[...]), pick)
    line = lax.broadcasted_iota(jnp.int32, (total, tall), 0)
    lane = lax.broadcasted_iota(jnp.int32, (total, tall), 1)
    named = line < 0
    for j in range(TOPK):
        named = named | (routes_wide[j : j + 1, :] == (line // block).astype(F32))
    up_row = lax.broadcasted_iota(jnp.int32, (tall, tall), 0)
    up_col = lax.broadcasted_iota(jnp.int32, (tall, tall), 1)
    same = up_row // count == up_col // count
    before = dot(onehot(named), onehot(same & (up_row < up_col)))
    fits = (before == (line % MOST).astype(F32)) & (lane // count == (line % block) // MOST)
    chosen = onehot(named & fits)
    smalls[1].wait()
    rows = second[...]
    stacked = jnp.concatenate([rows[:, q * part : (q + 1) * part] for q in range(PARTS)], 0)
    sbuf[...] = dot(chosen, stacked).astype(BF16).reshape(devices, block, part)
    pl.semaphore_wait(barrier, devices - 1)

    def remote(source, target, send, receive, peer):
        return pltpu.make_async_remote_copy(
            src_ref=source,
            dst_ref=target,
            send_sem=send,
            recv_sem=receive,
            device_id=(peer,),
            device_id_type=MESH,
        )

    before_me = lax.rem(group + groups - 1, groups) * GROUP + place
    after_me = lax.rem(group + 1, groups) * GROUP + place
    across_base = lax.rem(group + groups // 2, groups) * GROUP
    next_base = lax.rem(group + 1 + groups // 2, groups) * GROUP

    def hop(phase, source_ref):
        return remote(
            source_ref.at[pl.ds(across_base + GROUP - relayed, relayed)],
            hops.at[phase],
            send_sem.at[phase],
            hop_recv_sem.at[phase],
            before_me,
        )

    def start_all(phase, source_ref, target_ref):
        sent = send_sem.at[phase], recv_sem.at[phase]
        if relayed:
            hop(phase, source_ref).start()
        for far, near, peer in peers():
            if relayed and far == groups // 2:
                if near < GROUP - relayed:
                    peer = across_base + near
                    remote(source_ref.at[peer], target_ref.at[me], *sent, peer).start()
            else:
                remote(source_ref.at[peer], target_ref.at[me], *sent, peer).start()

    def forward(phase, source_ref, target_ref):
        if relayed:
            hop(phase, source_ref).wait_recv()
            for which in range(relayed):
                remote(
                    hops.at[phase, which],
                    target_ref.at[after_me],
                    hop_send_sem.at[phase],
                    recv_sem.at[phase],
                    next_base + GROUP - relayed + which,
                ).start()

    def everything(phase, source_ref, target_ref):
        others = pl.ds(0, devices - 1)
        return remote(
            source_ref.at[others],
            target_ref.at[others],
            send_sem.at[phase],
            recv_sem.at[phase],
            before_me,
        )

    def sent_all(phase, source_ref, target_ref):
        everything(phase, source_ref, target_ref).wait_send()
        if relayed:
            remote(
                hops.at[phase],
                target_ref.at[pl.ds(0, relayed)],
                hop_send_sem.at[phase],
                recv_sem.at[phase],
                before_me,
            ).wait_send()

    there = (0, sbuf, rbuf)
    back = (1, pbuf, abuf)
    start_all(*there)
    rbuf[me] = sbuf[me]

    smalls[2].wait()
    across = lax.broadcasted_iota(jnp.int32, (tall, total), 1)
    down = lax.broadcasted_iota(jnp.int32, (tall, total), 0)
    named_t = across < 0
    turned = (((1,), (1,)), ((), ()))
    lines_t = lax.broadcasted_iota(jnp.int32, (tall, routes.shape[1]), 1)
    lanes_t = lax.broadcasted_iota(jnp.int32, (tall, routes.shape[1]), 0)
    pick_t = onehot(lines_t == me * count + lanes_t % count)

    def picked(values):
        return lax.dot_general(pick_t, values, turned, preferred_element_type=F32)

    routes_tall = picked(onehot_values(routes[...]))
    weights_tall = sum(picked(piece) for piece in thirds(route_weights[...]))
    weight_t = jnp.zeros((tall, total), F32)
    for j in range(TOPK):
        hit = routes_tall[:, j : j + 1] == (across // block).astype(F32)
        named_t = named_t | hit
        weight_t = weight_t + jnp.where(hit, weights_tall[:, j : j + 1], 0.0)
    before_t = dot(onehot(same & (up_col < up_row)), onehot(named_t))
    fits_t = (before_t == (across % MOST).astype(F32)) & (
        down // count == (across % block) // MOST
    )
    weight_t = jnp.where(fits_t, weight_t, 0.0)
    weight_pieces = jnp.concatenate(thirds(weight_t), 0)

    forward(*there)

    def gated(inputs, gate_ref, up_ref):
        gate_part = dot(inputs, gate_ref[...])
        up_part = dot(inputs, up_ref[...])
        return (jax.nn.silu(gate_part) * up_part).astype(BF16)

    loads[0].wait()
    loads[1].wait()
    shared_hidden = gated(rows, sg, su)
    loads[2].wait()
    smalls[3].wait()
    kept = residual[...].astype(F32) + dot(shared_hidden, sd[...])

    slots = devices * MOST
    row = lax.broadcasted_iota(jnp.int32, (total, total), 0)
    col = lax.broadcasted_iota(jnp.int32, (total, total), 1)

    def ordered(place):
        return place % slots // MOST * block + place // slots * MOST + place % MOST

    take = onehot(col == ordered(row))
    give = onehot(row == ordered(col))

    for load in loads[3:]:
        load.wait()
    everything(*there).wait_recv()
    taken = dot(take, rbuf[...].reshape(total, part)).astype(BF16)
    for q in range(PARTS):
        xfull[:, q * part : (q + 1) * part] = taken[q * slots : (q + 1) * slots]
    hidden = gated(xfull[...], eg, eu)
    result = dot(hidden, ed[...]).astype(BF16)
    result = jnp.concatenate([result[:, q * part : (q + 1) * part] for q in range(PARTS)], 0)
    pbuf[...] = dot(give, result).astype(BF16).reshape(devices, block, part)
    start_all(*back)
    abuf[me] = pbuf[me]
    forward(*back)
    everything(*back).wait_recv()
    pieces = dot(weight_pieces, abuf[...].reshape(total, part))
    routed = pieces[:tall] + pieces[tall : 2 * tall] + pieces[2 * tall :]
    for q in range(PARTS):
        cut = slice(q * part, (q + 1) * part)
        out[:, cut] = (kept[:, cut] + routed[q * count : (q + 1) * count]).astype(BF16)
    sent_all(*there)
    sent_all(*back)


def experts(devices, second, residual, routes, weights, *matrices):
    count, width = second.shape
    vmem = pl.BlockSpec(memory_space=pltpu.VMEM)
    hbm = pl.BlockSpec(memory_space=pl.ANY)
    dma = pltpu.SemaphoreType.DMA
    exchange = pltpu.VMEM((devices, PARTS * MOST, width // PARTS), BF16)
    smalls = (second, residual, routes, weights)
    return pl.pallas_call(
        functools.partial(experts_kernel, devices),
        out_shape=jax.ShapeDtypeStruct((count, width), BF16),
        in_specs=[hbm] * 10,
        out_specs=vmem,
        scratch_shapes=[pltpu.VMEM(array.shape, array.dtype) for array in smalls]
        + [pltpu.VMEM(m.shape[-2:], BF16) for m in matrices]
        + [exchange] * 4
        + [
            pltpu.VMEM((2, GROUP // 2, PARTS * MOST, width // PARTS), BF16),
            pltpu.VMEM((devices * MOST, width), BF16),
            dma((4,)),
            dma((6,)),
            dma((2,)),
            dma((2,)),
            dma((2,)),
            dma((2,)),
        ],
        compiler_params=pltpu.CompilerParams(
            collective_id=1, has_side_effects=True, vmem_limit_bytes=VMEM_BYTES
        ),
        name="experts",
    )(*smalls, *matrices)


def per_device(
    tokens,
    recurrent_state,
    first_gain,
    w_receptance,
    w_key,
    w_value,
    decay_down,
    decay_up,
    decay_base,
    rate_down,
    rate_up,
    rate_base,
    key_scale,
    head_gain,
    w_output,
    second_gain,
    shared_gate,
    shared_up,
    shared_down,
    expert_gate,
    expert_up,
    expert_down,
    routes,
    route_weights,
):
    devices = lax.axis_size("ep")
    vectors = project(
        devices,
        (w_receptance, w_key, w_value),
        tokens,
        first_gain[None, :],
        decay_down.T,
        decay_up,
        decay_base[None, :],
        rate_down.T,
        rate_up,
        rate_base[None, :],
        key_scale[None, :],
    )
    new_state, residual, second = mixer(
        vectors,
        recurrent_state,
        head_gain[None, :],
        tokens,
        w_output,
        second_gain[None, :],
    )
    new_tokens = experts(
        devices,
        second,
        residual,
        routes.T,
        route_weights.T,
        shared_gate,
        shared_up,
        shared_down,
        expert_gate,
        expert_up,
        expert_down,
    )
    return (new_tokens, new_state)


def solution(mesh):
    in_specs = (
        P("ep", None),
        P("ep", None, None),
        P(),
        P("ep", None),
        P("ep", None),
        P("ep", None),
        P(),
        P(),
        P(),
        P(),
        P(),
        P(),
        P(),
        P(),
        P(),
        P(),
        P(),
        P(),
        P(),
        P("ep", None, None),
        P("ep", None, None),
        P("ep", None, None),
        P(),
        P(),
    )
    out_specs = (P("ep", None), P("ep", None, None))
    return jax.shard_map(
        per_device, mesh=mesh, in_specs=in_specs, out_specs=out_specs, check_vma=False
    )
```

```python
import functools

import jax
import jax.numpy as jnp
from jax import lax
from jax.experimental import pallas as pl
from jax.experimental.pallas import tpu as pltpu
from jax.sharding import PartitionSpec as P

HEAD = 64
TOPK = 4
MOST = 4
GROUP = 8
SPAN = 256
SPLIT = 2
NORM_EPS = 1e-06
GROUP_EPS = 0.00064
MESH = pl.DeviceIdType.MESH
F32 = jnp.float32
BF16 = jnp.bfloat16
VMEM_BYTES = 40 * 1024 * 1024


def dot(a, b):
    return jnp.dot(a, b, preferred_element_type=F32)


def rms_scale(inputs, gain):
    widened = inputs.astype(F32)
    return (
        widened * lax.rsqrt(jnp.mean(widened * widened, axis=-1, keepdims=True) + NORM_EPS) * gain
    )


def project_kernel(
    devices,
    tokens_in,
    gain_in,
    decay_down_in,
    decay_up_in,
    decay_base_in,
    rate_down_in,
    rate_up_in,
    rate_base_in,
    key_scale_in,
    w_r,
    w_k,
    w_v,
    state_in,
    w_output_in,
    head_gain_in,
    second_gain_in,
    routes_in,
    route_weights_in,
    out,
    tokens,
    state,
    w_output,
    head_gain,
    second_gain,
    routes,
    route_weights,
    gain,
    decay_down,
    decay_up,
    decay_base,
    rate_down,
    rate_up,
    rate_base,
    key_scale,
    stage,
    wbuf,
    nsend,
    xbuf,
    psend,
    precv,
    ahead_sem,
    small_sem,
    local_sem,
    wsend_sem,
    wrecv_sem,
    xsend_sem,
    xrecv_sem,
    psend_sem,
    precv_sem,
):
    rows, mix = w_r.shape
    half = mix // 2
    piece = half // SPLIT
    pieces = 3 * SPLIT
    count = tokens.shape[0]
    groups = devices // GROUP
    members = 2 * groups
    depth = tokens.shape[1] // groups
    me = lax.axis_index("ep")
    base = (me // GROUP) * GROUP
    place = me % GROUP
    core = me % 2
    column = place // 2
    member = (me // GROUP) * 2 + core
    chip = me - core
    x_bit = (place // 2) % 2
    y_bit = place // 4
    x_chip = chip + 2 - 4 * x_bit
    y_chip = chip + 4 - 8 * y_bit
    diag_chip = x_chip + 4 - 8 * y_bit
    partner = chip + 1 - core

    def peer_of(offset):
        which = (member + offset) % members
        return which, (which // 2) * GROUP + column * 2 + which % 2

    barrier = pltpu.get_barrier_semaphore()
    greet = [partner, x_chip, x_chip + 1, y_chip, y_chip + 1]
    greet = greet + [peer_of(offset)[1] for offset in range(1, members)]
    for peer in greet:
        pl.semaphore_signal(barrier, inc=1, device_id=(peer,), device_id_type=MESH)

    smalls = [
        pltpu.make_async_copy(source, target, small_sem.at[number])
        for number, (source, target) in enumerate(
            (
                (tokens_in, tokens),
                (gain_in, gain),
                (decay_down_in, decay_down),
                (decay_up_in, decay_up),
                (decay_base_in, decay_base),
                (rate_down_in, rate_down),
                (rate_up_in, rate_up),
                (rate_base_in, rate_base),
                (key_scale_in, key_scale),
            )
        )
    ]
    for small in smalls[:2]:
        small.start()
    for number, weight in enumerate((w_r, w_k, w_v)):
        for sub in range(SPLIT):
            for side in range(2):
                pltpu.make_async_copy(
                    weight.at[:, pl.ds(side * half + sub * piece, piece)],
                    stage.at[number * SPLIT + sub, side],
                    local_sem.at[number],
                ).start()
    for small in smalls[2:]:
        small.start()
    ahead = [
        pltpu.make_async_copy(source, target, ahead_sem.at[number])
        for number, (source, target) in enumerate(
            (
                (state_in, state),
                (w_output_in, w_output),
                (head_gain_in, head_gain),
                (second_gain_in, second_gain),
                (routes_in, routes),
                (route_weights_in, route_weights),
            )
        )
    ]
    for load in ahead:
        load.start()

    def loaded(number):
        span = stage.at[pl.ds(number * SPLIT, SPLIT)]
        pltpu.make_async_copy(span, span, local_sem.at[number]).wait()

    for small in smalls[:2]:
        small.wait()
    normed = rms_scale(tokens[...], gain[...]).astype(BF16)
    for number in range(groups):
        nsend[number] = normed[:, number * depth : (number + 1) * depth]
    loaded(0)
    pl.semaphore_wait(barrier, len(greet))

    def slot(number, device):
        return wbuf.at[number, pl.ds(pl.multiple_of((device - base) * rows, rows), rows), :]

    def remote(source, target, send, receive, device):
        return pltpu.make_async_remote_copy(
            src_ref=source,
            dst_ref=target,
            send_sem=send,
            recv_sem=receive,
            device_id=(device,),
            device_id_type=MESH,
        )

    def weight_copy(number, source, landing, kind, target):
        return remote(
            source, slot(number, landing), wsend_sem, wrecv_sem.at[number * 3 + kind], target
        )

    def direct(number):
        for side in range(2):
            source = stage.at[number, side]
            own_side = 1 - core
            weight_copy(number, source, me, core * 2, x_chip + side).start()
            weight_copy(number, source, me, own_side, y_chip + side).start()
        weight_copy(number, stage.at[number, 1 - core], me, 0, partner).start()

    def arrived(number, source, kind):
        weight_copy(number, stage.at[0, 0], source, kind, partner).wait_recv()

    def relay(number):
        arrived(number, y_chip, 1)
        weight_copy(number, slot(number, y_chip), y_chip, 0, x_chip + core).start()
        arrived(number, x_chip + 1, 2)
        weight_copy(number, slot(number, x_chip + 1), x_chip + 1, 0, y_chip + core).start()

    def rest(number):
        span = wbuf.at[number, pl.ds(0, 5 * rows), :]
        remote(span, span, wsend_sem, wrecv_sem.at[number * 3], partner).wait_recv()

    def own(number):
        mine = stage[number, core]
        wbuf[number, pl.ds(pl.multiple_of(place * rows, rows), rows), :] = mine

    direct(0)
    for offset in range(1, members):
        which, device = peer_of(offset)
        remote(nsend.at[which // 2], xbuf.at[member], xsend_sem, xrecv_sem, device).start()
    direct(1)
    loaded(1)
    direct(2)
    loaded(2)
    for number in range(pieces):
        own(number)
    xbuf[member] = nsend[me // GROUP]
    relay(0)
    direct(3)

    def put(number, values, first):
        for head in range(values.shape[1] // HEAD):
            out[number, :, first + head, :] = values[:, head * HEAD : (head + 1) * HEAD]

    heads = mix // HEAD
    flip = (((1,), (1,)), ((), ()))

    def down(matrix):
        return lax.dot_general(normed, matrix, flip, preferred_element_type=F32)

    for small in smalls[2:]:
        small.wait()
    decay_low = jnp.tanh(down(decay_down[...])).astype(BF16)
    decay_pre = decay_base[...] + dot(decay_low, decay_up[...])
    put(3, jnp.exp(-jnp.exp(-jax.nn.softplus(-decay_pre) - 0.5)), 0)
    relay(1)
    direct(4)
    rate_low = down(rate_down[...]).astype(BF16)
    put(4, jax.nn.sigmoid(rate_base[...] + dot(rate_low, rate_up[...])), 0)
    relay(2)
    direct(5)

    others = pl.ds(0, members - 1)
    remote(xbuf.at[others], xbuf.at[others], xsend_sem, xrecv_sem, partner).wait_recv()
    stacked = xbuf[...].reshape(members * count, depth)

    def multiply(number):
        rest(number)
        part = dot(stacked, wbuf[number]).astype(BF16)
        psend[number] = part.reshape(members, count, piece)
        for offset in range(1, members):
            which, device = peer_of(offset)
            remote(
                psend.at[number, which],
                precv.at[number, member],
                psend_sem,
                precv_sem.at[number],
                device,
            ).start()
        precv[number, member] = psend[number, member]

    def finish(number):
        span = precv.at[number, others]
        remote(span, span, psend_sem, precv_sem.at[number], partner).wait_recv()
        for side in range(2):
            total = precv[number, side].astype(F32)
            for which in range(1, groups):
                total = total + precv[number, which * 2 + side].astype(F32)
            total = total.astype(BF16).astype(F32)
            column = side * half + number % SPLIT * piece
            put(number // SPLIT, total, column // HEAD)
            if number // SPLIT == 1:
                put(5, total * key_scale[:, column : column + piece], column // HEAD)

    multiply(0)
    relay(3)
    multiply(1)
    relay(4)
    multiply(2)
    relay(5)
    finish(0)
    multiply(3)
    finish(1)
    multiply(4)
    finish(2)
    multiply(5)
    finish(3)
    finish(4)
    finish(5)
    span = wbuf.at[:, pl.ds(0, 7 * rows), :]
    remote(span, span, wsend_sem, wrecv_sem.at[0], partner).wait_send()
    remote(xbuf.at[others], xbuf.at[others], xsend_sem, xrecv_sem, partner).wait_send()
    span = psend.at[:, others]
    remote(span, span, psend_sem, precv_sem.at[0], partner).wait_send()
    for load in ahead:
        load.wait()


def project(devices, weights, aheads, *smalls):
    count, width = smalls[0].shape
    rows, mix = weights[0].shape
    groups = devices // GROUP
    members = 2 * groups
    piece = mix // 2 // SPLIT
    pieces = 3 * SPLIT
    vmem = pl.BlockSpec(memory_space=pltpu.VMEM)
    hbm = pl.BlockSpec(memory_space=pltpu.HBM)
    dma = pltpu.SemaphoreType.DMA
    return pl.pallas_call(
        functools.partial(project_kernel, devices),
        out_shape=[pltpu.VMEM((6, count, mix // HEAD, HEAD), F32)]
        + [pltpu.VMEM(array.shape, array.dtype) for array in (smalls[0],) + aheads],
        in_specs=[hbm] * (12 + len(aheads)),
        out_specs=[vmem] * (2 + len(aheads)),
        scratch_shapes=[pltpu.VMEM(array.shape, array.dtype) for array in smalls[1:]]
        + [
            pltpu.VMEM((pieces, 2, rows, piece), BF16),
            pltpu.VMEM((pieces, GROUP * rows, piece), BF16),
            pltpu.VMEM((groups, count, width // groups), BF16),
            pltpu.VMEM((members, count, width // groups), BF16),
            pltpu.VMEM((pieces, members, count, piece), BF16),
            pltpu.VMEM((pieces, members, count, piece), BF16),
            dma((len(aheads),)),
            dma((9,)),
            dma((3,)),
            dma,
            dma((3 * pieces,)),
            dma,
            dma,
            dma,
            dma((pieces,)),
        ],
        compiler_params=pltpu.CompilerParams(
            collective_id=0, has_side_effects=True, vmem_limit_bytes=VMEM_BYTES
        ),
        name="project",
    )(*map(pinned, (*smalls, *weights, *aheads)))


def split_sum(values, ones):
    high = values.astype(BF16)
    low = (values - high.astype(F32)).astype(BF16)
    return dot(high, ones) + dot(low, ones)


def mixer_kernel(
    steps,
    vectors,
    state,
    head_gain,
    tokens,
    w_output,
    second_gain,
    new_state,
    residual,
    second,
    fresh_out,
    mixed,
    work,
    sums,
    out_sem,
):
    _, count, heads, _ = vectors.shape
    entries = state.shape[2]
    per_step = count // steps
    span = SPAN
    tiles = entries // span
    copies = span // HEAD

    def rows_of(step):
        return pl.ds(step * per_step, per_step)

    row = lax.broadcasted_iota(jnp.int32, (span, span), 0)
    col = lax.broadcasted_iota(jnp.int32, (span, span), 1)
    ones = (row // HEAD == col // HEAD).astype(F32).astype(BF16)
    lane = lax.broadcasted_iota(jnp.int32, (heads, span), 1)

    def widen(inputs):
        return jnp.concatenate([inputs] * copies, axis=1)

    def one_step(step, carry):
        size = tiles * heads
        kept = []
        for place in range(per_step):
            number = step * per_step + place
            reader, keys, values, decay, learn, scaled = [vectors[w, number] for w in range(6)]
            direction = scaled / jnp.sqrt(jnp.sum(scaled * scaled, axis=-1, keepdims=True) + 1.0)
            learned = direction * learn
            wide_direction = widen(direction)
            wide_values = widen(values)
            wide_reader = widen(reader * decay)
            base = place * 3 * size
            for i in range(tiles):
                block = state[number, :, i * span : (i + 1) * span]
                pick = lane % HEAD == i * copies + lane // HEAD
                part = slice(base + i * heads, base + (i + 1) * heads)
                work[part] = (block * wide_direction).astype(BF16)
                part = slice(base + size + i * heads, base + size + (i + 1) * heads)
                work[part] = jnp.where(pick, wide_values, 0.0).astype(BF16)
                product = block * wide_reader
                high = product.astype(BF16)
                part = slice(base + 2 * size + i * heads, base + 2 * size + (i + 1) * heads)
                work[part] = high
            along_learned = jnp.sum(learned * reader, axis=-1, keepdims=True)
            along_keys = jnp.sum(keys * reader, axis=-1, keepdims=True)
            kept.append(
                (number, base, widen(decay), widen(learned), widen(keys))
                + (along_learned, along_keys, values)
            )
        sums[...] = dot(work[...], ones)
        for number, base, wide_decay, wide_learn, wide_keys, along_learned, along_keys, values in kept:
            picked_removed = jnp.zeros((heads, span), F32)
            picked_read = jnp.zeros((heads, span), F32)
            for i in range(tiles):
                block = state[number, :, i * span : (i + 1) * span]
                pick = lane % HEAD == i * copies + lane // HEAD

                def summed(which):
                    first = base + which * size + i * heads
                    return sums[first : first + heads]

                removed = summed(0)
                fresh_out[number, :, i * span : (i + 1) * span] = (
                    block * wide_decay - removed * wide_learn + summed(1) * wide_keys
                )
                picked_removed = jnp.where(pick, removed, picked_removed)
                picked_read = jnp.where(pick, summed(2), picked_read)
            picked = picked_read - picked_removed * along_learned
            readout = values * along_keys
            for i in range(copies):
                readout = readout + picked[:, i * HEAD : (i + 1) * HEAD]
            centre = jnp.mean(readout, axis=-1, keepdims=True)
            spread = jnp.mean(jnp.square(readout - centre), axis=-1, keepdims=True)
            mixed[number] = (readout - centre) * lax.rsqrt(spread + GROUP_EPS)
        pltpu.make_async_copy(
            fresh_out.at[rows_of(step)], new_state.at[rows_of(step)], out_sem
        ).start()
        return carry

    lax.fori_loop(0, steps, one_step, 0)

    channels = heads * HEAD
    flat = mixed[...].reshape(count * heads, HEAD)
    source = lax.broadcasted_iota(jnp.int32, (HEAD, channels), 0)
    target = lax.broadcasted_iota(jnp.int32, (HEAD, channels), 1)
    tiled = split_sum(flat, (target % HEAD == source).astype(F32).astype(BF16))
    head = lax.broadcasted_iota(jnp.int32, (count * heads, channels), 0) % heads
    channel = lax.broadcasted_iota(jnp.int32, (count * heads, channels), 1) // HEAD
    kept = (jnp.where(head == channel, tiled, 0.0) * head_gain[...]).astype(BF16)
    owner = lax.broadcasted_iota(jnp.int32, (count, count * heads), 1) // heads
    token = lax.broadcasted_iota(jnp.int32, (count, count * heads), 0)
    rows = dot((owner == token).astype(F32).astype(BF16), kept).astype(BF16)
    after = (tokens[...].astype(F32) + dot(rows, w_output[...])).astype(BF16)
    residual[...] = after
    second[...] = rms_scale(after, second_gain[...]).astype(BF16)
    pltpu.make_async_copy(fresh_out, new_state, out_sem).wait()


def mixer(vectors, state, head_gain, tokens, w_output, second_gain):
    _, count, heads, _ = vectors.shape
    width = tokens.shape[1]
    per_step = 8 if count % 8 == 0 else 1
    steps = count // per_step
    rows = per_step * 3 * state.shape[1] * (state.shape[2] // SPAN)
    vmem = pl.BlockSpec(memory_space=pltpu.VMEM)
    hbm = pl.BlockSpec(memory_space=pl.ANY)
    dma = pltpu.SemaphoreType.DMA
    return pl.pallas_call(
        functools.partial(mixer_kernel, steps),
        out_shape=[
            jax.ShapeDtypeStruct(state.shape, F32),
            pltpu.VMEM((count, width), BF16),
            pltpu.VMEM((count, width), BF16),
        ],
        in_specs=[vmem] * 6,
        out_specs=[hbm, vmem, vmem],
        scratch_shapes=[
            pltpu.VMEM(state.shape, F32),
            pltpu.VMEM((count, heads, HEAD), F32),
            pltpu.VMEM((rows, SPAN), BF16),
            pltpu.VMEM((rows, SPAN), F32),
            dma,
        ],
        compiler_params=pltpu.CompilerParams(vmem_limit_bytes=VMEM_BYTES),
        name="mixer",
    )(vectors, state, head_gain, tokens, w_output, second_gain)


def onehot(flags):
    return flags.astype(F32).astype(BF16)


def onehot_values(values):
    return values.astype(F32).astype(BF16)


def thirds(values):
    first = values.astype(BF16)
    rest = values - first.astype(F32)
    middle = rest.astype(BF16)
    return first, middle, (rest - middle.astype(F32)).astype(BF16)


def experts_kernel(
    devices,
    second,
    residual,
    routes,
    route_weights,
    shared_gate,
    shared_up,
    shared_down,
    expert_gate,
    expert_up,
    expert_down,
    out,
    sg,
    su,
    sd,
    eg,
    eu,
    ed,
    sbuf,
    rbuf,
    pbuf,
    abuf,
    local_sem,
    send_sem,
    recv_sem,
):
    count, width = second.shape
    total = devices * MOST
    groups = devices // GROUP
    me = lax.axis_index("ep")
    group = me // GROUP
    place = me % GROUP
    barrier = pltpu.get_barrier_semaphore()
    def peers():
        order = sorted(range(groups), key=lambda g: (-min(g, groups - g), g))
        for far in order:
            base = lax.rem(group + far, groups) * GROUP
            for near in range(GROUP):
                if far or near:
                    yield base + lax.rem(place + near, GROUP)

    for peer in peers():
        pl.semaphore_signal(barrier, inc=1, device_id=(peer,), device_id_type=MESH)
    loads = [
        pltpu.make_async_copy(source, target, local_sem.at[number])
        for number, (source, target) in enumerate(
            (
                (shared_gate, sg),
                (shared_up, su),
                (shared_down, sd),
                (expert_gate.at[0], eg),
                (expert_up.at[0], eu),
                (expert_down.at[0], ed),
            )
        )
    ]
    for load in loads:
        load.start()

    lines = lax.broadcasted_iota(jnp.int32, (routes.shape[1], count), 0)
    lanes = lax.broadcasted_iota(jnp.int32, (routes.shape[1], count), 1)
    pick = onehot(lines == me * count + lanes)
    routes_wide = dot(onehot_values(routes[...]), pick)
    line = lax.broadcasted_iota(jnp.int32, (total, count), 0)
    named = line < 0
    for j in range(TOPK):
        named = named | (routes_wide[j : j + 1, :] == (line // MOST).astype(F32))
    up_row = lax.broadcasted_iota(jnp.int32, (count, count), 0)
    up_col = lax.broadcasted_iota(jnp.int32, (count, count), 1)
    before = dot(onehot(named), onehot(up_row < up_col))
    chosen = onehot(named & (before == (line % MOST).astype(F32)))
    rows = second[...]
    sbuf[...] = dot(chosen, rows).astype(BF16).reshape(devices, MOST, width)
    pl.semaphore_wait(barrier, devices - 1)

    def remote(source, target, send, receive, peer):
        return pltpu.make_async_remote_copy(
            src_ref=source,
            dst_ref=target,
            send_sem=send,
            recv_sem=receive,
            device_id=(peer,),
            device_id_type=MESH,
        )

    def start_all(phase, source_ref, target_ref):
        for peer in peers():
            remote(
                source_ref.at[peer],
                target_ref.at[me],
                send_sem.at[phase],
                recv_sem.at[phase],
                peer,
            ).start()

    def everything(phase, source_ref, target_ref):
        others = pl.ds(0, devices - 1)
        return remote(
            source_ref.at[others],
            target_ref.at[others],
            send_sem.at[phase],
            recv_sem.at[phase],
            lax.rem(me + 1, devices),
        )

    there = (0, sbuf, rbuf)
    back = (1, pbuf, abuf)
    start_all(*there)
    rbuf[me] = sbuf[me]

    across = lax.broadcasted_iota(jnp.int32, (count, total), 1)
    named_t = across < 0
    turned = (((1,), (1,)), ((), ()))
    lines_t = lax.broadcasted_iota(jnp.int32, (count, routes.shape[1]), 1)
    lanes_t = lax.broadcasted_iota(jnp.int32, (count, routes.shape[1]), 0)
    pick_t = onehot(lines_t == me * count + lanes_t)

    def picked(values):
        return lax.dot_general(pick_t, values, turned, preferred_element_type=F32)

    routes_tall = picked(onehot_values(routes[...]))
    weights_tall = sum(picked(piece) for piece in thirds(route_weights[...]))
    weight_t = jnp.zeros((count, total), F32)
    for j in range(TOPK):
        hit = routes_tall[:, j : j + 1] == (across // MOST).astype(F32)
        named_t = named_t | hit
        weight_t = weight_t + jnp.where(hit, weights_tall[:, j : j + 1], 0.0)
    before_t = dot(onehot(up_col < up_row), onehot(named_t))
    weight_t = jnp.where(before_t == (across % MOST).astype(F32), weight_t, 0.0)
    weight_pieces = jnp.concatenate(thirds(weight_t), 0)

    def gated(inputs, gate_ref, up_ref):
        gate_part = dot(inputs, gate_ref[...])
        up_part = dot(inputs, up_ref[...])
        return (jax.nn.silu(gate_part) * up_part).astype(BF16)

    loads[0].wait()
    loads[1].wait()
    shared_hidden = gated(rows, sg, su)
    loads[2].wait()
    kept = residual[...].astype(F32) + dot(shared_hidden, sd[...])

    for load in loads[3:]:
        load.wait()
    everything(*there).wait_recv()
    hidden = gated(rbuf[...].reshape(total, width), eg, eu)
    pbuf[...] = dot(hidden, ed[...]).astype(BF16).reshape(devices, MOST, width)
    start_all(*back)
    abuf[me] = pbuf[me]
    everything(*back).wait_recv()
    pieces = dot(weight_pieces, abuf[...].reshape(total, width))
    routed = pieces[:count] + pieces[count : 2 * count] + pieces[2 * count :]
    out[...] = (kept + routed).astype(BF16)
    everything(*there).wait_send()
    everything(*back).wait_send()


def experts(devices, second, residual, routes, weights, *matrices):
    count, width = second.shape
    vmem = pl.BlockSpec(memory_space=pltpu.VMEM)
    hbm = pl.BlockSpec(memory_space=pltpu.HBM)
    dma = pltpu.SemaphoreType.DMA
    exchange = pltpu.VMEM((devices, MOST, width), BF16)
    return pl.pallas_call(
        functools.partial(experts_kernel, devices),
        out_shape=pltpu.VMEM((count, width), BF16),
        in_specs=[vmem] * 4 + [hbm] * 6,
        out_specs=vmem,
        scratch_shapes=[pltpu.VMEM(m.shape[-2:], BF16) for m in matrices]
        + [exchange] * 4
        + [
            dma((6,)),
            dma((2,)),
            dma((2,)),
        ],
        compiler_params=pltpu.CompilerParams(
            collective_id=1, has_side_effects=True, vmem_limit_bytes=VMEM_BYTES
        ),
        name="experts",
    )(second, residual, routes, weights, *map(pinned, matrices))


def pinned(array):
    return pltpu.with_memory_space_constraint(array, pltpu.HBM)


def per_device(
    tokens,
    recurrent_state,
    first_gain,
    w_receptance,
    w_key,
    w_value,
    decay_down,
    decay_up,
    decay_base,
    rate_down,
    rate_up,
    rate_base,
    key_scale,
    head_gain,
    w_output,
    second_gain,
    shared_gate,
    shared_up,
    shared_down,
    expert_gate,
    expert_up,
    expert_down,
    routes,
    route_weights,
):
    devices = lax.axis_size("ep")
    vectors, *ahead = project(
        devices,
        (w_receptance, w_key, w_value),
        (
            recurrent_state,
            w_output,
            head_gain[None, :],
            second_gain[None, :],
            routes.T,
            route_weights.T,
        ),
        tokens,
        first_gain[None, :],
        decay_down.T,
        decay_up,
        decay_base[None, :],
        rate_down.T,
        rate_up,
        rate_base[None, :],
        key_scale[None, :],
    )
    tokens, state, w_output, head_gain, second_gain, routes, route_weights = ahead
    new_state, residual, second = mixer(vectors, state, head_gain, tokens, w_output, second_gain)
    new_tokens = experts(
        devices,
        second,
        residual,
        routes,
        route_weights,
        shared_gate,
        shared_up,
        shared_down,
        expert_gate,
        expert_up,
        expert_down,
    )
    return (new_tokens, new_state)


def solution(mesh):
    in_specs = (
        P("ep", None),
        P("ep", None, None),
        P(),
        P("ep", None),
        P("ep", None),
        P("ep", None),
        P(),
        P(),
        P(),
        P(),
        P(),
        P(),
        P(),
        P(),
        P(),
        P(),
        P(),
        P(),
        P(),
        P("ep", None, None),
        P("ep", None, None),
        P("ep", None, None),
        P(),
        P(),
    )
    out_specs = (P("ep", None), P("ep", None, None))
    return jax.shard_map(
        per_device, mesh=mesh, in_specs=in_specs, out_specs=out_specs, check_vma=False
    )
```

```python
import functools

import jax
import jax.numpy as jnp
from jax import lax
from jax.experimental import pallas as pl
from jax.experimental.pallas import tpu as pltpu
from jax.sharding import PartitionSpec as P

HEAD = 64
TOPK = 4
MOST = 4
GROUP = 8
SPAN = 256
SPLIT = 2
NORM_EPS = 1e-06
GROUP_EPS = 0.00064
MESH = pl.DeviceIdType.MESH
F32 = jnp.float32
BF16 = jnp.bfloat16
VMEM_BYTES = 57 * 1024 * 1024
CLOSE_BYTES = 16 * 1024 * 1024


def dot(a, b):
    return jnp.dot(a, b, preferred_element_type=F32)


def rms_scale(inputs, gain):
    widened = inputs.astype(F32)
    return (
        widened * lax.rsqrt(jnp.mean(widened * widened, axis=-1, keepdims=True) + NORM_EPS) * gain
    )


def project_kernel(
    devices,
    tokens_in,
    gain_in,
    decay_down_in,
    decay_up_in,
    decay_base_in,
    rate_down_in,
    rate_up_in,
    rate_base_in,
    key_scale_in,
    w_r,
    w_k,
    w_v,
    state_in,
    w_output_in,
    head_gain_in,
    second_gain_in,
    routes_in,
    route_weights_in,
    out,
    tokens,
    state,
    w_output,
    head_gain,
    second_gain,
    routes,
    route_weights,
    gain,
    decay_down,
    decay_up,
    decay_base,
    rate_down,
    rate_up,
    rate_base,
    key_scale,
    stage,
    wbuf,
    nsend,
    xbuf,
    psend,
    precv,
    ahead_sem,
    small_sem,
    local_sem,
    wsend_sem,
    wrecv_sem,
    xsend_sem,
    xrecv_sem,
    psend_sem,
    precv_sem,
    between,
):
    rows, mix = w_r.shape
    half = mix // 2
    piece = half // SPLIT
    pieces = 3 * SPLIT
    count = tokens.shape[0]
    groups = devices // GROUP
    members = 2 * groups
    depth = tokens.shape[1] // groups
    me = lax.axis_index("ep")
    base = (me // GROUP) * GROUP
    place = me % GROUP
    core = me % 2
    column = place // 2
    member = (me // GROUP) * 2 + core
    chip = me - core
    x_bit = (place // 2) % 2
    y_bit = place // 4
    x_chip = chip + 2 - 4 * x_bit
    y_chip = chip + 4 - 8 * y_bit
    diag_chip = x_chip + 4 - 8 * y_bit
    partner = chip + 1 - core

    def peer_of(offset):
        which = (member + offset) % members
        return which, (which // 2) * GROUP + column * 2 + which % 2

    barrier = pltpu.get_barrier_semaphore()
    greet = [partner, x_chip, x_chip + 1, y_chip, y_chip + 1]
    greet = greet + [peer_of(offset)[1] for offset in range(1, members)]
    for peer in greet:
        pl.semaphore_signal(barrier, inc=1, device_id=(peer,), device_id_type=MESH)

    smalls = [
        pltpu.make_async_copy(source, target, small_sem.at[number])
        for number, (source, target) in enumerate(
            (
                (tokens_in, tokens),
                (gain_in, gain),
                (decay_down_in, decay_down),
                (decay_up_in, decay_up),
                (decay_base_in, decay_base),
                (rate_down_in, rate_down),
                (rate_up_in, rate_up),
                (rate_base_in, rate_base),
                (key_scale_in, key_scale),
            )
        )
    ]
    for small in smalls[:2]:
        small.start()
    for number, weight in enumerate((w_r, w_k, w_v)):
        for sub in range(SPLIT):
            for side in range(2):
                pltpu.make_async_copy(
                    weight.at[:, pl.ds(side * half + sub * piece, piece)],
                    stage.at[number * SPLIT + sub, side],
                    local_sem.at[number],
                ).start()
    for small in smalls[2:]:
        small.start()
    ahead = [
        pltpu.make_async_copy(source, target, ahead_sem.at[number])
        for number, (source, target) in enumerate(
            (
                (state_in, state),
                (w_output_in, w_output),
                (head_gain_in, head_gain),
                (second_gain_in, second_gain),
                (routes_in, routes),
                (route_weights_in, route_weights),
            )
        )
    ]
    for load in ahead:
        load.start()

    def loaded(number):
        span = stage.at[pl.ds(number * SPLIT, SPLIT)]
        pltpu.make_async_copy(span, span, local_sem.at[number]).wait()

    for small in smalls[:2]:
        small.wait()
    normed = rms_scale(tokens[...], gain[...]).astype(BF16)
    for number in range(groups):
        nsend[number] = normed[:, number * depth : (number + 1) * depth]
    loaded(0)
    pl.semaphore_wait(barrier, len(greet))

    def slot(number, device):
        return wbuf.at[number, pl.ds(pl.multiple_of((device - base) * rows, rows), rows), :]

    def remote(source, target, send, receive, device):
        return pltpu.make_async_remote_copy(
            src_ref=source,
            dst_ref=target,
            send_sem=send,
            recv_sem=receive,
            device_id=(device,),
            device_id_type=MESH,
        )

    def weight_copy(number, source, landing, kind, target):
        return remote(
            source, slot(number, landing), wsend_sem, wrecv_sem.at[number * 3 + kind], target
        )

    def direct(number):
        for side in range(2):
            source = stage.at[number, side]
            own_side = 1 - core
            weight_copy(number, source, me, core * 2, x_chip + side).start()
            weight_copy(number, source, me, own_side, y_chip + side).start()
        weight_copy(number, stage.at[number, 1 - core], me, 0, partner).start()

    def arrived(number, source, kind):
        weight_copy(number, stage.at[0, 0], source, kind, partner).wait_recv()

    def relay(number):
        arrived(number, y_chip, 1)
        weight_copy(number, slot(number, y_chip), y_chip, 0, x_chip + core).start()
        arrived(number, x_chip + 1, 2)
        weight_copy(number, slot(number, x_chip + 1), x_chip + 1, 0, y_chip + core).start()

    def rest(number):
        span = wbuf.at[number, pl.ds(0, 5 * rows), :]
        remote(span, span, wsend_sem, wrecv_sem.at[number * 3], partner).wait_recv()

    def own(number):
        mine = stage[number, core]
        wbuf[number, pl.ds(pl.multiple_of(place * rows, rows), rows), :] = mine

    direct(0)
    for offset in range(1, members):
        which, device = peer_of(offset)
        remote(nsend.at[which // 2], xbuf.at[member], xsend_sem, xrecv_sem, device).start()
    direct(1)
    loaded(1)
    direct(2)
    loaded(2)
    for number in range(pieces):
        own(number)
    xbuf[member] = nsend[me // GROUP]
    relay(0)
    direct(3)

    def put(number, values, first):
        for head in range(values.shape[1] // HEAD):
            out[number, :, first + head, :] = values[:, head * HEAD : (head + 1) * HEAD]

    heads = mix // HEAD
    flip = (((1,), (1,)), ((), ()))

    def down(matrix):
        return lax.dot_general(normed, matrix, flip, preferred_element_type=F32)

    for small in smalls[2:]:
        small.wait()
    decay_low = jnp.tanh(down(decay_down[...])).astype(BF16)
    decay_pre = decay_base[...] + dot(decay_low, decay_up[...])
    put(3, jnp.exp(-jnp.exp(-jax.nn.softplus(-decay_pre) - 0.5)), 0)
    relay(1)
    direct(4)
    rate_low = down(rate_down[...]).astype(BF16)
    put(4, jax.nn.sigmoid(rate_base[...] + dot(rate_low, rate_up[...])), 0)
    relay(2)
    direct(5)
    for load in ahead[4:]:
        load.wait()
    between()

    others = pl.ds(0, members - 1)
    remote(xbuf.at[others], xbuf.at[others], xsend_sem, xrecv_sem, partner).wait_recv()
    stacked = xbuf[...].reshape(members * count, depth)

    def multiply(number):
        rest(number)
        part = dot(stacked, wbuf[number]).astype(BF16)
        psend[number] = part.reshape(members, count, piece)
        for offset in range(1, members):
            which, device = peer_of(offset)
            remote(
                psend.at[number, which],
                precv.at[number, member],
                psend_sem,
                precv_sem.at[number],
                device,
            ).start()
        precv[number, member] = psend[number, member]

    def finish(number):
        span = precv.at[number, others]
        remote(span, span, psend_sem, precv_sem.at[number], partner).wait_recv()
        for side in range(2):
            total = precv[number, side].astype(F32)
            for which in range(1, groups):
                total = total + precv[number, which * 2 + side].astype(F32)
            total = total.astype(BF16).astype(F32)
            column = side * half + number % SPLIT * piece
            put(number // SPLIT, total, column // HEAD)
            if number // SPLIT == 1:
                put(5, total * key_scale[:, column : column + piece], column // HEAD)

    multiply(0)
    relay(3)
    multiply(1)
    relay(4)
    multiply(2)
    relay(5)
    finish(0)
    multiply(3)
    finish(1)
    multiply(4)
    finish(2)
    multiply(5)
    finish(3)
    finish(4)
    finish(5)
    span = wbuf.at[:, pl.ds(0, 7 * rows), :]
    remote(span, span, wsend_sem, wrecv_sem.at[0], partner).wait_send()
    remote(xbuf.at[others], xbuf.at[others], xsend_sem, xrecv_sem, partner).wait_send()
    span = psend.at[:, others]
    remote(span, span, psend_sem, precv_sem.at[0], partner).wait_send()
    for load in ahead[:4]:
        load.wait()


def split_sum(values, ones):
    high = values.astype(BF16)
    low = (values - high.astype(F32)).astype(BF16)
    return dot(high, ones) + dot(low, ones)


def mixer_setup(vectors, state):
    _, count, heads, _ = vectors.shape
    tiles = state.shape[2] // SPAN
    copies = SPAN // HEAD
    lane = lax.broadcasted_iota(jnp.int32, (heads, SPAN), 1)

    def widen(inputs):
        return jnp.concatenate([inputs] * copies, axis=1)

    def pick(i):
        return lane % HEAD == i * copies + lane // HEAD

    def directed(number):
        scaled = vectors[5, number]
        return scaled / jnp.sqrt(jnp.sum(scaled * scaled, axis=-1, keepdims=True) + 1.0)

    return count, heads, tiles, copies, widen, pick, directed


def mixer_read(vectors, state, head_gain, tokens, w_output, second_gain, mixed, work, sums):
    count, heads, tiles, copies, widen, pick, directed = mixer_setup(vectors, state)
    steps = sums.shape[0]
    per_step = count // steps
    size = tiles * heads
    row = lax.broadcasted_iota(jnp.int32, (SPAN, SPAN), 0)
    col = lax.broadcasted_iota(jnp.int32, (SPAN, SPAN), 1)
    ones = (row // HEAD == col // HEAD).astype(F32).astype(BF16)

    def one_step(step, carry):
        kept = []
        for place in range(per_step):
            number = step * per_step + place
            reader, keys, values, decay, learn = [vectors[w, number] for w in range(5)]
            direction = directed(number)
            learned = direction * learn
            wide_direction = widen(direction)
            wide_values = widen(values)
            wide_reader = widen(reader * decay)
            base = place * 3 * size
            for i in range(tiles):
                block = state[number, :, i * SPAN : (i + 1) * SPAN]
                first = base + i * heads
                work[first : first + heads] = (block * wide_direction).astype(BF16)
                first = first + size
                work[first : first + heads] = jnp.where(pick(i), wide_values, 0.0).astype(BF16)
                first = first + size
                work[first : first + heads] = (block * wide_reader).astype(BF16)
            along_learned = jnp.sum(learned * reader, axis=-1, keepdims=True)
            along_keys = jnp.sum(keys * reader, axis=-1, keepdims=True)
            kept.append((number, base, along_learned, along_keys, values))
        sums[step] = dot(work[...], ones)
        for number, base, along_learned, along_keys, values in kept:
            picked_removed = jnp.zeros((heads, SPAN), F32)
            picked_read = jnp.zeros((heads, SPAN), F32)
            for i in range(tiles):
                first = base + i * heads
                picked_removed = jnp.where(
                    pick(i), sums[step, first : first + heads], picked_removed
                )
                first = first + 2 * size
                picked_read = jnp.where(pick(i), sums[step, first : first + heads], picked_read)
            picked = picked_read - picked_removed * along_learned
            readout = values * along_keys
            for i in range(copies):
                readout = readout + picked[:, i * HEAD : (i + 1) * HEAD]
            centre = jnp.mean(readout, axis=-1, keepdims=True)
            spread = jnp.mean(jnp.square(readout - centre), axis=-1, keepdims=True)
            mixed[number] = (readout - centre) * lax.rsqrt(spread + GROUP_EPS)
        return carry

    lax.fori_loop(0, steps, one_step, 0)

    channels = heads * HEAD
    flat = mixed[...].reshape(count * heads, HEAD)
    source = lax.broadcasted_iota(jnp.int32, (HEAD, channels), 0)
    target = lax.broadcasted_iota(jnp.int32, (HEAD, channels), 1)
    tiled = split_sum(flat, (target % HEAD == source).astype(F32).astype(BF16))
    head = lax.broadcasted_iota(jnp.int32, (count * heads, channels), 0) % heads
    channel = lax.broadcasted_iota(jnp.int32, (count * heads, channels), 1) // HEAD
    kept = (jnp.where(head == channel, tiled, 0.0) * head_gain[...]).astype(BF16)
    owner = lax.broadcasted_iota(jnp.int32, (count, count * heads), 1) // heads
    token = lax.broadcasted_iota(jnp.int32, (count, count * heads), 0)
    rows = dot((owner == token).astype(F32).astype(BF16), kept).astype(BF16)
    after = (tokens[...].astype(F32) + dot(rows, w_output[...])).astype(BF16)
    return after, rms_scale(after, second_gain[...]).astype(BF16)


def mixer_update(vectors, state, sums, new_state):
    count, heads, tiles, copies, widen, pick, directed = mixer_setup(vectors, state)
    steps = sums.shape[0]
    per_step = count // steps
    size = tiles * heads

    def one_token(number, carry):
        keys, decay, learn = vectors[1, number], vectors[3, number], vectors[4, number]
        wide_decay = widen(decay)
        wide_learn = widen(directed(number) * learn)
        wide_keys = widen(keys)
        step = number // per_step
        base = number % per_step * (3 * size)

        def summed(i, which):
            first = pl.multiple_of(base + which * size + i * heads, heads)
            return sums[step, pl.ds(first, heads), :]

        for i in range(tiles):
            block = state[number, :, i * SPAN : (i + 1) * SPAN]
            new_state[number, :, i * SPAN : (i + 1) * SPAN] = (
                block * wide_decay - summed(i, 0) * wide_learn + summed(i, 1) * wide_keys
            )
        return carry

    lax.fori_loop(0, count, one_token, 0)


def onehot(flags):
    return flags.astype(F32).astype(BF16)


def onehot_values(values):
    return values.astype(F32).astype(BF16)


def thirds(values):
    first = values.astype(BF16)
    rest = values - first.astype(F32)
    middle = rest.astype(BF16)
    return first, middle, (rest - middle.astype(F32)).astype(BF16)


def plan_routes(devices, routes, route_weights, chosen, pieces_out):
    total, count = chosen.shape
    me = lax.axis_index("ep")
    lines = lax.broadcasted_iota(jnp.int32, (routes.shape[1], count), 0)
    lanes = lax.broadcasted_iota(jnp.int32, (routes.shape[1], count), 1)
    pick = onehot(lines == me * count + lanes)
    routes_wide = dot(onehot_values(routes[...]), pick)
    line = lax.broadcasted_iota(jnp.int32, (total, count), 0)
    named = line < 0
    for j in range(TOPK):
        named = named | (routes_wide[j : j + 1, :] == (line // MOST).astype(F32))
    up_row = lax.broadcasted_iota(jnp.int32, (count, count), 0)
    up_col = lax.broadcasted_iota(jnp.int32, (count, count), 1)
    before = dot(onehot(named), onehot(up_row < up_col))
    chosen[...] = onehot(named & (before == (line % MOST).astype(F32)))
    across = lax.broadcasted_iota(jnp.int32, (count, total), 1)
    named_t = across < 0
    turned = (((1,), (1,)), ((), ()))
    lines_t = lax.broadcasted_iota(jnp.int32, (count, routes.shape[1]), 1)
    lanes_t = lax.broadcasted_iota(jnp.int32, (count, routes.shape[1]), 0)
    pick_t = onehot(lines_t == me * count + lanes_t)

    def picked(values):
        return lax.dot_general(pick_t, values, turned, preferred_element_type=F32)

    routes_tall = picked(onehot_values(routes[...]))
    weights_tall = sum(picked(piece) for piece in thirds(route_weights[...]))
    weight_t = jnp.zeros((count, total), F32)
    for j in range(TOPK):
        hit = routes_tall[:, j : j + 1] == (across // MOST).astype(F32)
        named_t = named_t | hit
        weight_t = weight_t + jnp.where(hit, weights_tall[:, j : j + 1], 0.0)
    before_t = dot(onehot(up_col < up_row), onehot(named_t))
    weight_t = jnp.where(before_t == (across % MOST).astype(F32), weight_t, 0.0)
    pieces_out[...] = jnp.concatenate(thirds(weight_t), 0)


def experts_kernel(
    devices,
    second,
    residual,
    chosen,
    loads,
    kept_out,
    abuf,
    sg,
    su,
    sd,
    eg,
    eu,
    ed,
    sbuf,
    rbuf,
    pbuf,
    send_sem,
    recv_sem,
    meet,
    between,
):
    count, width = second.shape
    total = devices * MOST
    groups = devices // GROUP
    me = lax.axis_index("ep")
    group = me // GROUP
    place = me % GROUP
    def peers():
        order = sorted(range(groups), key=lambda g: (-min(g, groups - g), g))
        for far in order:
            base = lax.rem(group + far, groups) * GROUP
            for near in range(GROUP):
                if far or near:
                    yield base + lax.rem(place + near, GROUP)

    rows = second
    sbuf[...] = dot(chosen[...], rows).astype(BF16).reshape(devices, MOST, width)
    meet()

    def remote(source, target, send, receive, peer):
        return pltpu.make_async_remote_copy(
            src_ref=source,
            dst_ref=target,
            send_sem=send,
            recv_sem=receive,
            device_id=(peer,),
            device_id_type=MESH,
        )

    def start_all(phase, source_ref, target_ref):
        for peer in peers():
            remote(
                source_ref.at[peer],
                target_ref.at[me],
                send_sem.at[phase],
                recv_sem.at[phase],
                peer,
            ).start()

    def everything(phase, source_ref, target_ref):
        others = pl.ds(0, devices - 1)
        return remote(
            source_ref.at[others],
            target_ref.at[others],
            send_sem.at[phase],
            recv_sem.at[phase],
            lax.rem(me + 1, devices),
        )

    there = (0, sbuf, rbuf)
    back = (1, pbuf, abuf)
    start_all(*there)
    rbuf[me] = sbuf[me]
    between()

    def gated(inputs, gate_ref, up_ref):
        gate_part = dot(inputs, gate_ref[...])
        up_part = dot(inputs, up_ref[...])
        return (jax.nn.silu(gate_part) * up_part).astype(BF16)

    loads[0].wait()
    loads[1].wait()
    shared_hidden = gated(rows, sg, su)
    loads[2].wait()
    kept_out[...] = residual.astype(F32) + dot(shared_hidden, sd[...])

    for load in loads[3:]:
        load.wait()
    everything(*there).wait_recv()
    hidden = gated(rbuf[...].reshape(total, width), eg, eu)
    pbuf[...] = dot(hidden, ed[...]).astype(BF16).reshape(devices, MOST, width)
    start_all(*back)
    abuf[me] = pbuf[me]
    everything(*back).wait_recv()
    everything(*there).wait_send()
    everything(*back).wait_send()


def layer_kernel(devices, refs):
    (
        ins,
        matrices,
        kept_out,
        pieces_out,
        answers,
        new_state,
        chosen,
        vectors,
        held,
        project_scratch,
        mixed,
        work,
        sums,
        expert_scratch,
        local_sem,
    ) = refs
    tokens, state, w_output, head_gain, second_gain, routes, route_weights = held
    project_kernel(
        devices,
        *ins,
        vectors,
        *held,
        *project_scratch,
        lambda: plan_routes(devices, routes, route_weights, chosen, pieces_out),
    )
    me = lax.axis_index("ep")
    barrier = pltpu.get_barrier_semaphore()
    for offset in range(1, devices):
        pl.semaphore_signal(
            barrier, inc=1, device_id=(lax.rem(me + offset, devices),), device_id_type=MESH
        )
    loads = []
    for number, (source, target) in enumerate(zip(matrices, expert_scratch[:6])):
        source = source.at[0] if number >= 3 else source
        loads.append(pltpu.make_async_copy(source, target, local_sem.at[number]))
        loads[-1].start()
    residual, second = mixer_read(
        vectors, state, head_gain, tokens, w_output, second_gain, mixed, work, sums
    )
    experts_kernel(
        devices,
        second,
        residual,
        chosen,
        loads,
        kept_out,
        answers,
        *expert_scratch,
        lambda: pl.semaphore_wait(barrier, devices - 1),
        lambda: mixer_update(vectors, state, sums, new_state),
    )


def layer(devices, smalls, weights, aheads, matrices):
    tokens, state, w_output = smalls[0], aheads[0], aheads[1]
    count, width = tokens.shape
    rows, mix = weights[0].shape
    heads = mix // HEAD
    groups = devices // GROUP
    members = 2 * groups
    piece = mix // 2 // SPLIT
    pieces = 3 * SPLIT
    steps = count // 8 if count % 8 == 0 else 1
    lines = count // steps * 3 * heads * (state.shape[2] // SPAN)
    vmem = pl.BlockSpec(memory_space=pltpu.VMEM)
    hbm = pl.BlockSpec(memory_space=pltpu.HBM)
    dma = pltpu.SemaphoreType.DMA
    exchange = pltpu.VMEM((devices, MOST, width), BF16)
    project_scratch = [pltpu.VMEM(array.shape, array.dtype) for array in smalls[1:]] + [
        pltpu.VMEM((pieces, 2, rows, piece), BF16),
        pltpu.VMEM((pieces, GROUP * rows, piece), BF16),
        pltpu.VMEM((groups, count, width // groups), BF16),
        pltpu.VMEM((members, count, width // groups), BF16),
        pltpu.VMEM((pieces, members, count, piece), BF16),
        pltpu.VMEM((pieces, members, count, piece), BF16),
        dma((len(aheads),)),
        dma((9,)),
        dma((3,)),
        dma,
        dma((3 * pieces,)),
        dma,
        dma,
        dma,
        dma((pieces,)),
    ]
    expert_scratch = (
        [pltpu.VMEM(m.shape[-2:], BF16) for m in matrices] + [exchange] * 3 + [dma((2,))] * 2
    )
    held = [pltpu.VMEM(array.shape, array.dtype) for array in (tokens,) + aheads]
    shapes = [
        [None] * (len(smalls) + len(weights) + len(aheads)),
        [None] * len(matrices),
        None,
        None,
        None,
        None,
        pltpu.VMEM((devices * MOST, count), BF16),
        pltpu.VMEM((6, count, heads, HEAD), F32),
        held,
        project_scratch,
        pltpu.VMEM((count, heads, HEAD), F32),
        pltpu.VMEM((lines, SPAN), BF16),
        pltpu.VMEM((steps, lines, SPAN), F32),
        expert_scratch,
        dma((len(matrices),)),
    ]

    def kernel(*flat):
        rest = iter(flat)
        layer_kernel(
            devices,
            [[next(rest) for _ in s] if isinstance(s, list) else next(rest) for s in shapes],
        )

    scratch = []
    for shape in shapes[6:]:
        scratch.extend(shape if isinstance(shape, list) else [shape])
    operands = (*smalls, *weights, *aheads, *matrices)
    return pl.pallas_call(
        kernel,
        out_shape=[
            pltpu.VMEM((count, width), F32),
            pltpu.VMEM((3 * count, devices * MOST), BF16),
            exchange,
            pltpu.VMEM(state.shape, F32),
        ],
        in_specs=[hbm] * len(operands),
        out_specs=[vmem] * 4,
        scratch_shapes=scratch,
        compiler_params=pltpu.CompilerParams(
            collective_id=0, has_side_effects=True, vmem_limit_bytes=VMEM_BYTES
        ),
        name="layer",
    )(*map(pinned, operands))


def close_kernel(kept, weight_pieces, answers, state, out, new_state, mixed, sem, out_sem):
    count = kept.shape[0]
    chunks = sem.shape[0]
    copies = []
    for number in range(chunks):
        span = pl.ds(number * (count // chunks), count // chunks)
        copies.append(pltpu.make_async_copy(state.at[span], new_state.at[span], sem.at[number]))
        copies[-1].start()
    total = weight_pieces.shape[1]
    pieces = dot(weight_pieces[...], answers[...].reshape(total, kept.shape[1]))
    routed = pieces[:count] + pieces[count : 2 * count] + pieces[2 * count :]
    mixed[...] = (kept[...] + routed).astype(BF16)
    copies.append(pltpu.make_async_copy(mixed, out, out_sem))
    copies[-1].start()
    for copy in copies:
        copy.wait()


def close(kept, weight_pieces, answers, state):
    vmem = pl.BlockSpec(memory_space=pltpu.VMEM)
    hbm = pl.BlockSpec(memory_space=pltpu.HBM)
    return pl.pallas_call(
        close_kernel,
        out_shape=[
            jax.ShapeDtypeStruct(kept.shape, BF16),
            jax.ShapeDtypeStruct(state.shape, F32),
        ],
        in_specs=[vmem] * 4,
        out_specs=[hbm, hbm],
        scratch_shapes=[
            pltpu.VMEM(kept.shape, BF16),
            pltpu.SemaphoreType.DMA((8 if state.shape[0] % 8 == 0 else 1,)),
            pltpu.SemaphoreType.DMA,
        ],
        compiler_params=pltpu.CompilerParams(vmem_limit_bytes=CLOSE_BYTES),
        name="close",
    )(kept, weight_pieces, answers, state)


def pinned(array):
    return pltpu.with_memory_space_constraint(array, pltpu.HBM)


def per_device(
    tokens,
    recurrent_state,
    first_gain,
    w_receptance,
    w_key,
    w_value,
    decay_down,
    decay_up,
    decay_base,
    rate_down,
    rate_up,
    rate_base,
    key_scale,
    head_gain,
    w_output,
    second_gain,
    shared_gate,
    shared_up,
    shared_down,
    expert_gate,
    expert_up,
    expert_down,
    routes,
    route_weights,
):
    devices = lax.axis_size("ep")
    results = layer(
        devices,
        (
            tokens,
            first_gain[None, :],
            decay_down.T,
            decay_up,
            decay_base[None, :],
            rate_down.T,
            rate_up,
            rate_base[None, :],
            key_scale[None, :],
        ),
        (w_receptance, w_key, w_value),
        (
            recurrent_state,
            w_output,
            head_gain[None, :],
            second_gain[None, :],
            routes.T,
            route_weights.T,
        ),
        (shared_gate, shared_up, shared_down, expert_gate, expert_up, expert_down),
    )
    return close(*results)


def solution(mesh):
    in_specs = (
        P("ep", None),
        P("ep", None, None),
        P(),
        P("ep", None),
        P("ep", None),
        P("ep", None),
        P(),
        P(),
        P(),
        P(),
        P(),
        P(),
        P(),
        P(),
        P(),
        P(),
        P(),
        P(),
        P(),
        P("ep", None, None),
        P("ep", None, None),
        P("ep", None, None),
        P(),
        P(),
    )
    out_specs = (P("ep", None), P("ep", None, None))
    return jax.shard_map(
        per_device, mesh=mesh, in_specs=in_specs, out_specs=out_specs, check_vma=False
    )
```

```python
import functools

import jax
import jax.numpy as jnp
from jax import lax
from jax.experimental import pallas as pl
from jax.experimental.pallas import tpu as pltpu
from jax.sharding import PartitionSpec as P

HEAD = 64
TOPK = 4
MOST = 4
GROUP = 8
SPAN = 256
SPLIT = 2
NORM_EPS = 1e-06
GROUP_EPS = 0.00064
MESH = pl.DeviceIdType.MESH
F32 = jnp.float32
BF16 = jnp.bfloat16
VMEM_BYTES = 57 * 1024 * 1024
CLOSE_BYTES = 16 * 1024 * 1024


def dot(a, b):
    return jnp.dot(a, b, preferred_element_type=F32)


def rms_scale(inputs, gain):
    widened = inputs.astype(F32)
    return (
        widened * lax.rsqrt(jnp.mean(widened * widened, axis=-1, keepdims=True) + NORM_EPS) * gain
    )


def project_kernel(
    devices,
    tokens_in,
    gain_in,
    decay_down_in,
    decay_up_in,
    decay_base_in,
    rate_down_in,
    rate_up_in,
    rate_base_in,
    key_scale_in,
    w_r,
    w_k,
    w_v,
    state_in,
    w_output_in,
    head_gain_in,
    second_gain_in,
    routes_in,
    route_weights_in,
    out,
    tokens,
    state,
    w_output,
    head_gain,
    second_gain,
    routes,
    route_weights,
    gain,
    decay_down,
    decay_up,
    decay_base,
    rate_down,
    rate_up,
    rate_base,
    key_scale,
    stage,
    wbuf,
    nsend,
    xbuf,
    psend,
    precv,
    ahead_sem,
    small_sem,
    local_sem,
    wsend_sem,
    wrecv_sem,
    xsend_sem,
    xrecv_sem,
    psend_sem,
    precv_sem,
    between,
):
    rows, mix = w_r.shape
    half = mix // 2
    piece = half // SPLIT
    pieces = 3 * SPLIT
    count = tokens.shape[0]
    groups = devices // GROUP
    members = 2 * groups
    depth = tokens.shape[1] // groups
    me = lax.axis_index("ep")
    base = (me // GROUP) * GROUP
    place = me % GROUP
    core = me % 2
    column = place // 2
    member = (me // GROUP) * 2 + core
    chip = me - core
    x_bit = (place // 2) % 2
    y_bit = place // 4
    x_chip = chip + 2 - 4 * x_bit
    y_chip = chip + 4 - 8 * y_bit
    diag_chip = x_chip + 4 - 8 * y_bit
    partner = chip + 1 - core

    def peer_of(offset):
        which = (member + offset) % members
        return which, (which // 2) * GROUP + column * 2 + which % 2

    barrier = pltpu.get_barrier_semaphore()
    greet = [partner, x_chip, x_chip + 1, y_chip, y_chip + 1]
    greet = greet + [peer_of(offset)[1] for offset in range(1, members)]
    for peer in greet:
        pl.semaphore_signal(barrier, inc=1, device_id=(peer,), device_id_type=MESH)

    smalls = [
        pltpu.make_async_copy(source, target, small_sem.at[number])
        for number, (source, target) in enumerate(
            (
                (tokens_in, tokens),
                (gain_in, gain),
                (decay_down_in, decay_down),
                (decay_up_in, decay_up),
                (decay_base_in, decay_base),
                (rate_down_in, rate_down),
                (rate_up_in, rate_up),
                (rate_base_in, rate_base),
                (key_scale_in, key_scale),
            )
        )
    ]
    for small in smalls[:2]:
        small.start()
    for number, weight in enumerate((w_r, w_k, w_v)):
        for sub in range(SPLIT):
            for side in range(2):
                pltpu.make_async_copy(
                    weight.at[:, pl.ds(side * half + sub * piece, piece)],
                    stage.at[number * SPLIT + sub, side],
                    local_sem.at[number],
                ).start()
    for small in smalls[2:]:
        small.start()
    ahead = [
        pltpu.make_async_copy(source, target, ahead_sem.at[number])
        for number, (source, target) in enumerate(
            (
                (state_in, state),
                (w_output_in, w_output),
                (head_gain_in, head_gain),
                (second_gain_in, second_gain),
                (routes_in, routes),
                (route_weights_in, route_weights),
            )
        )
    ]
    for load in ahead:
        load.start()

    def loaded(number):
        span = stage.at[pl.ds(number * SPLIT, SPLIT)]
        pltpu.make_async_copy(span, span, local_sem.at[number]).wait()

    for small in smalls[:2]:
        small.wait()
    normed = rms_scale(tokens[...], gain[...]).astype(BF16)
    for number in range(groups):
        nsend[number] = normed[:, number * depth : (number + 1) * depth]
    loaded(0)
    pl.semaphore_wait(barrier, len(greet))

    def slot(number, device):
        return wbuf.at[number, pl.ds(pl.multiple_of((device - base) * rows, rows), rows), :]

    def remote(source, target, send, receive, device):
        return pltpu.make_async_remote_copy(
            src_ref=source,
            dst_ref=target,
            send_sem=send,
            recv_sem=receive,
            device_id=(device,),
            device_id_type=MESH,
        )

    def weight_copy(number, source, landing, kind, target):
        return remote(
            source, slot(number, landing), wsend_sem, wrecv_sem.at[number * 3 + kind], target
        )

    def direct(number):
        for side in range(2):
            source = stage.at[number, side]
            own_side = 1 - core
            weight_copy(number, source, me, core * 2, x_chip + side).start()
            weight_copy(number, source, me, own_side, y_chip + side).start()
        weight_copy(number, stage.at[number, 1 - core], me, 0, partner).start()

    def arrived(number, source, kind):
        weight_copy(number, stage.at[0, 0], source, kind, partner).wait_recv()

    def relay(number):
        arrived(number, y_chip, 1)
        weight_copy(number, slot(number, y_chip), y_chip, 0, x_chip + core).start()
        arrived(number, x_chip + 1, 2)
        weight_copy(number, slot(number, x_chip + 1), x_chip + 1, 0, y_chip + core).start()

    def rest(number):
        span = wbuf.at[number, pl.ds(0, 5 * rows), :]
        remote(span, span, wsend_sem, wrecv_sem.at[number * 3], partner).wait_recv()

    def own(number):
        mine = stage[number, core]
        wbuf[number, pl.ds(pl.multiple_of(place * rows, rows), rows), :] = mine

    direct(0)
    for offset in range(1, members):
        which, device = peer_of(offset)
        remote(nsend.at[which // 2], xbuf.at[member], xsend_sem, xrecv_sem, device).start()
    direct(1)
    loaded(1)
    direct(2)
    loaded(2)
    for number in range(pieces):
        own(number)
    xbuf[member] = nsend[me // GROUP]
    relay(0)
    direct(3)

    def put(number, values, first):
        for head in range(values.shape[1] // HEAD):
            out[number, :, first + head, :] = values[:, head * HEAD : (head + 1) * HEAD]

    heads = mix // HEAD
    flip = (((1,), (1,)), ((), ()))

    def down(matrix):
        return lax.dot_general(normed, matrix, flip, preferred_element_type=F32)

    for small in smalls[2:]:
        small.wait()
    decay_low = jnp.tanh(down(decay_down[...])).astype(BF16)
    decay_pre = decay_base[...] + dot(decay_low, decay_up[...])
    put(3, jnp.exp(-jnp.exp(-jax.nn.softplus(-decay_pre) - 0.5)), 0)
    relay(1)
    direct(4)
    rate_low = down(rate_down[...]).astype(BF16)
    put(4, jax.nn.sigmoid(rate_base[...] + dot(rate_low, rate_up[...])), 0)
    relay(2)
    direct(5)
    for load in ahead[4:]:
        load.wait()
    between()

    others = pl.ds(0, members - 1)
    remote(xbuf.at[others], xbuf.at[others], xsend_sem, xrecv_sem, partner).wait_recv()
    stacked = xbuf[...].reshape(members * count, depth)

    def multiply(number):
        rest(number)
        part = dot(stacked, wbuf[number]).astype(BF16)
        psend[number] = part.reshape(members, count, piece)
        for offset in range(1, members):
            which, device = peer_of(offset)
            remote(
                psend.at[number, which],
                precv.at[number, member],
                psend_sem,
                precv_sem.at[number],
                device,
            ).start()
        precv[number, member] = psend[number, member]

    def finish(number):
        span = precv.at[number, others]
        remote(span, span, psend_sem, precv_sem.at[number], partner).wait_recv()
        for side in range(2):
            total = precv[number, side].astype(F32)
            for which in range(1, groups):
                total = total + precv[number, which * 2 + side].astype(F32)
            total = total.astype(BF16).astype(F32)
            column = side * half + number % SPLIT * piece
            put(number // SPLIT, total, column // HEAD)
            if number // SPLIT == 1:
                put(5, total * key_scale[:, column : column + piece], column // HEAD)

    multiply(0)
    relay(3)
    multiply(1)
    relay(4)
    multiply(2)
    relay(5)
    finish(0)
    multiply(3)
    finish(1)
    multiply(4)
    finish(2)
    multiply(5)
    finish(3)
    finish(4)
    finish(5)
    span = wbuf.at[:, pl.ds(0, 7 * rows), :]
    remote(span, span, wsend_sem, wrecv_sem.at[0], partner).wait_send()
    remote(xbuf.at[others], xbuf.at[others], xsend_sem, xrecv_sem, partner).wait_send()
    span = psend.at[:, others]
    remote(span, span, psend_sem, precv_sem.at[0], partner).wait_send()
    for load in ahead[:4]:
        load.wait()


def split_sum(values, ones):
    high = values.astype(BF16)
    low = (values - high.astype(F32)).astype(BF16)
    return dot(high, ones) + dot(low, ones)


def mixer_setup(vectors, state):
    _, count, heads, _ = vectors.shape
    tiles = state.shape[2] // SPAN
    copies = SPAN // HEAD
    lane = lax.broadcasted_iota(jnp.int32, (heads, SPAN), 1)

    def widen(inputs):
        return jnp.concatenate([inputs] * copies, axis=1)

    def pick(i):
        return lane % HEAD == i * copies + lane // HEAD

    def directed(number):
        scaled = vectors[5, number]
        return scaled / jnp.sqrt(jnp.sum(scaled * scaled, axis=-1, keepdims=True) + 1.0)

    return count, heads, tiles, copies, widen, pick, directed


def mixer_read(vectors, state, head_gain, tokens, w_output, second_gain, mixed, work, sums):
    count, heads, tiles, copies, widen, pick, directed = mixer_setup(vectors, state)
    steps = sums.shape[0]
    per_step = count // steps
    size = tiles * heads
    row = lax.broadcasted_iota(jnp.int32, (SPAN, SPAN), 0)
    col = lax.broadcasted_iota(jnp.int32, (SPAN, SPAN), 1)
    ones = (row // HEAD == col // HEAD).astype(F32).astype(BF16)

    def one_step(step, carry):
        kept = []
        for place in range(per_step):
            number = step * per_step + place
            reader, keys, values, decay, learn = [vectors[w, number] for w in range(5)]
            direction = directed(number)
            learned = direction * learn
            wide_direction = widen(direction)
            wide_values = widen(values)
            wide_reader = widen(reader * decay)
            base = place * 3 * size
            for i in range(tiles):
                block = state[number, :, i * SPAN : (i + 1) * SPAN]
                first = base + i * heads
                work[first : first + heads] = (block * wide_direction).astype(BF16)
                first = first + size
                work[first : first + heads] = jnp.where(pick(i), wide_values, 0.0).astype(BF16)
                first = first + size
                work[first : first + heads] = (block * wide_reader).astype(BF16)
            along_learned = jnp.sum(learned * reader, axis=-1, keepdims=True)
            along_keys = jnp.sum(keys * reader, axis=-1, keepdims=True)
            kept.append((number, base, along_learned, along_keys, values))
        sums[step] = dot(work[...], ones)
        for number, base, along_learned, along_keys, values in kept:
            picked_removed = jnp.zeros((heads, SPAN), F32)
            picked_read = jnp.zeros((heads, SPAN), F32)
            for i in range(tiles):
                first = base + i * heads
                picked_removed = jnp.where(
                    pick(i), sums[step, first : first + heads], picked_removed
                )
                first = first + 2 * size
                picked_read = jnp.where(pick(i), sums[step, first : first + heads], picked_read)
            picked = picked_read - picked_removed * along_learned
            readout = values * along_keys
            for i in range(copies):
                readout = readout + picked[:, i * HEAD : (i + 1) * HEAD]
            centre = jnp.mean(readout, axis=-1, keepdims=True)
            spread = jnp.mean(jnp.square(readout - centre), axis=-1, keepdims=True)
            mixed[number] = (readout - centre) * lax.rsqrt(spread + GROUP_EPS)
        return carry

    lax.fori_loop(0, steps, one_step, 0)

    channels = heads * HEAD
    flat = mixed[...].reshape(count * heads, HEAD)
    source = lax.broadcasted_iota(jnp.int32, (HEAD, channels), 0)
    target = lax.broadcasted_iota(jnp.int32, (HEAD, channels), 1)
    tiled = split_sum(flat, (target % HEAD == source).astype(F32).astype(BF16))
    head = lax.broadcasted_iota(jnp.int32, (count * heads, channels), 0) % heads
    channel = lax.broadcasted_iota(jnp.int32, (count * heads, channels), 1) // HEAD
    kept = (jnp.where(head == channel, tiled, 0.0) * head_gain[...]).astype(BF16)
    owner = lax.broadcasted_iota(jnp.int32, (count, count * heads), 1) // heads
    token = lax.broadcasted_iota(jnp.int32, (count, count * heads), 0)
    rows = dot((owner == token).astype(F32).astype(BF16), kept).astype(BF16)
    after = (tokens[...].astype(F32) + dot(rows, w_output[...])).astype(BF16)
    return after, rms_scale(after, second_gain[...]).astype(BF16)


def mixer_update(vectors, state, sums, new_state):
    count, heads, tiles, copies, widen, pick, directed = mixer_setup(vectors, state)
    steps = sums.shape[0]
    per_step = count // steps
    size = tiles * heads

    def one_token(number, carry):
        keys, decay, learn = vectors[1, number], vectors[3, number], vectors[4, number]
        wide_decay = widen(decay)
        wide_learn = widen(directed(number) * learn)
        wide_keys = widen(keys)
        step = number // per_step
        base = number % per_step * (3 * size)

        def summed(i, which):
            first = pl.multiple_of(base + which * size + i * heads, heads)
            return sums[step, pl.ds(first, heads), :]

        for i in range(tiles):
            block = state[number, :, i * SPAN : (i + 1) * SPAN]
            new_state[number, :, i * SPAN : (i + 1) * SPAN] = (
                block * wide_decay - summed(i, 0) * wide_learn + summed(i, 1) * wide_keys
            )
        return carry

    lax.fori_loop(0, count, one_token, 0)


def onehot(flags):
    return flags.astype(F32).astype(BF16)


def onehot_values(values):
    return values.astype(F32).astype(BF16)


def thirds(values):
    first = values.astype(BF16)
    rest = values - first.astype(F32)
    middle = rest.astype(BF16)
    return first, middle, (rest - middle.astype(F32)).astype(BF16)


def plan_routes(devices, routes, route_weights, chosen, pieces_out):
    total, count = chosen.shape
    me = lax.axis_index("ep")
    lines = lax.broadcasted_iota(jnp.int32, (routes.shape[1], count), 0)
    lanes = lax.broadcasted_iota(jnp.int32, (routes.shape[1], count), 1)
    pick = onehot(lines == me * count + lanes)
    routes_wide = dot(onehot_values(routes[...]), pick)
    line = lax.broadcasted_iota(jnp.int32, (total, count), 0)
    named = line < 0
    for j in range(TOPK):
        named = named | (routes_wide[j : j + 1, :] == (line // MOST).astype(F32))
    up_row = lax.broadcasted_iota(jnp.int32, (count, count), 0)
    up_col = lax.broadcasted_iota(jnp.int32, (count, count), 1)
    before = dot(onehot(named), onehot(up_row < up_col))
    chosen[...] = onehot(named & (before == (line % MOST).astype(F32)))
    across = lax.broadcasted_iota(jnp.int32, (count, total), 1)
    named_t = across < 0
    turned = (((1,), (1,)), ((), ()))
    lines_t = lax.broadcasted_iota(jnp.int32, (count, routes.shape[1]), 1)
    lanes_t = lax.broadcasted_iota(jnp.int32, (count, routes.shape[1]), 0)
    pick_t = onehot(lines_t == me * count + lanes_t)

    def picked(values):
        return lax.dot_general(pick_t, values, turned, preferred_element_type=F32)

    routes_tall = picked(onehot_values(routes[...]))
    weights_tall = sum(picked(piece) for piece in thirds(route_weights[...]))
    weight_t = jnp.zeros((count, total), F32)
    for j in range(TOPK):
        hit = routes_tall[:, j : j + 1] == (across // MOST).astype(F32)
        named_t = named_t | hit
        weight_t = weight_t + jnp.where(hit, weights_tall[:, j : j + 1], 0.0)
    before_t = dot(onehot(up_col < up_row), onehot(named_t))
    weight_t = jnp.where(before_t == (across % MOST).astype(F32), weight_t, 0.0)
    pieces_out[...] = jnp.concatenate(thirds(weight_t), 0)


def experts_kernel(
    devices,
    second,
    residual,
    chosen,
    loads,
    kept_out,
    abuf,
    sg,
    su,
    sd,
    eg,
    eu,
    ed,
    sbuf,
    rbuf,
    pbuf,
    send_sem,
    recv_sem,
    meet,
    between,
):
    count, width = second.shape
    total = devices * MOST
    groups = devices // GROUP
    me = lax.axis_index("ep")
    group = me // GROUP
    place = me % GROUP
    def peers():
        order = sorted(range(groups), key=lambda g: (-min(g, groups - g), g))
        for far in order:
            turned = far + (1 - group % 2) * (groups - 2 * far) if far else far
            base = lax.rem(group + turned, groups) * GROUP
            for near in range(GROUP):
                if far or near:
                    yield base + lax.rem(place + near, GROUP)

    rows = second
    sbuf[...] = dot(chosen[...], rows).astype(BF16).reshape(devices, MOST, width)
    meet()

    def remote(source, target, send, receive, peer):
        return pltpu.make_async_remote_copy(
            src_ref=source,
            dst_ref=target,
            send_sem=send,
            recv_sem=receive,
            device_id=(peer,),
            device_id_type=MESH,
        )

    def start_all(phase, source_ref, target_ref):
        for peer in peers():
            remote(
                source_ref.at[peer],
                target_ref.at[me],
                send_sem.at[phase],
                recv_sem.at[phase],
                peer,
            ).start()

    def everything(phase, source_ref, target_ref):
        others = pl.ds(0, devices - 1)
        return remote(
            source_ref.at[others],
            target_ref.at[others],
            send_sem.at[phase],
            recv_sem.at[phase],
            lax.rem(me + 1, devices),
        )

    there = (0, sbuf, rbuf)
    back = (1, pbuf, abuf)
    start_all(*there)
    rbuf[me] = sbuf[me]
    between()

    def gated(inputs, gate_ref, up_ref):
        gate_part = dot(inputs, gate_ref[...])
        up_part = dot(inputs, up_ref[...])
        return (jax.nn.silu(gate_part) * up_part).astype(BF16)

    loads[0].wait()
    loads[1].wait()
    shared_hidden = gated(rows, sg, su)
    loads[2].wait()
    kept_out[...] = residual.astype(F32) + dot(shared_hidden, sd[...])

    for load in loads[3:]:
        load.wait()
    everything(*there).wait_recv()
    hidden = gated(rbuf[...].reshape(total, width), eg, eu)
    pbuf[...] = dot(hidden, ed[...]).astype(BF16).reshape(devices, MOST, width)
    start_all(*back)
    abuf[me] = pbuf[me]
    everything(*back).wait_recv()
    everything(*there).wait_send()
    everything(*back).wait_send()


def layer_kernel(devices, refs):
    (
        ins,
        matrices,
        kept_out,
        pieces_out,
        answers,
        new_state,
        chosen,
        vectors,
        held,
        project_scratch,
        mixed,
        work,
        sums,
        expert_scratch,
        local_sem,
    ) = refs
    tokens, state, w_output, head_gain, second_gain, routes, route_weights = held
    project_kernel(
        devices,
        *ins,
        vectors,
        *held,
        *project_scratch,
        lambda: plan_routes(devices, routes, route_weights, chosen, pieces_out),
    )
    me = lax.axis_index("ep")
    barrier = pltpu.get_barrier_semaphore()
    for offset in range(1, devices):
        pl.semaphore_signal(
            barrier, inc=1, device_id=(lax.rem(me + offset, devices),), device_id_type=MESH
        )
    loads = []
    for number, (source, target) in enumerate(zip(matrices, expert_scratch[:6])):
        source = source.at[0] if number >= 3 else source
        loads.append(pltpu.make_async_copy(source, target, local_sem.at[number]))
        loads[-1].start()
    residual, second = mixer_read(
        vectors, state, head_gain, tokens, w_output, second_gain, mixed, work, sums
    )
    experts_kernel(
        devices,
        second,
        residual,
        chosen,
        loads,
        kept_out,
        answers,
        *expert_scratch,
        lambda: pl.semaphore_wait(barrier, devices - 1),
        lambda: mixer_update(vectors, state, sums, new_state),
    )


def layer(devices, smalls, weights, aheads, matrices):
    tokens, state, w_output = smalls[0], aheads[0], aheads[1]
    count, width = tokens.shape
    rows, mix = weights[0].shape
    heads = mix // HEAD
    groups = devices // GROUP
    members = 2 * groups
    piece = mix // 2 // SPLIT
    pieces = 3 * SPLIT
    steps = count // 8 if count % 8 == 0 else 1
    lines = count // steps * 3 * heads * (state.shape[2] // SPAN)
    vmem = pl.BlockSpec(memory_space=pltpu.VMEM)
    hbm = pl.BlockSpec(memory_space=pltpu.HBM)
    dma = pltpu.SemaphoreType.DMA
    exchange = pltpu.VMEM((devices, MOST, width), BF16)
    project_scratch = [pltpu.VMEM(array.shape, array.dtype) for array in smalls[1:]] + [
        pltpu.VMEM((pieces, 2, rows, piece), BF16),
        pltpu.VMEM((pieces, GROUP * rows, piece), BF16),
        pltpu.VMEM((groups, count, width // groups), BF16),
        pltpu.VMEM((members, count, width // groups), BF16),
        pltpu.VMEM((pieces, members, count, piece), BF16),
        pltpu.VMEM((pieces, members, count, piece), BF16),
        dma((len(aheads),)),
        dma((9,)),
        dma((3,)),
        dma,
        dma((3 * pieces,)),
        dma,
        dma,
        dma,
        dma((pieces,)),
    ]
    expert_scratch = (
        [pltpu.VMEM(m.shape[-2:], BF16) for m in matrices] + [exchange] * 3 + [dma((2,))] * 2
    )
    held = [pltpu.VMEM(array.shape, array.dtype) for array in (tokens,) + aheads]
    shapes = [
        [None] * (len(smalls) + len(weights) + len(aheads)),
        [None] * len(matrices),
        None,
        None,
        None,
        None,
        pltpu.VMEM((devices * MOST, count), BF16),
        pltpu.VMEM((6, count, heads, HEAD), F32),
        held,
        project_scratch,
        pltpu.VMEM((count, heads, HEAD), F32),
        pltpu.VMEM((lines, SPAN), BF16),
        pltpu.VMEM((steps, lines, SPAN), F32),
        expert_scratch,
        dma((len(matrices),)),
    ]

    def kernel(*flat):
        rest = iter(flat)
        layer_kernel(
            devices,
            [[next(rest) for _ in s] if isinstance(s, list) else next(rest) for s in shapes],
        )

    scratch = []
    for shape in shapes[6:]:
        scratch.extend(shape if isinstance(shape, list) else [shape])
    operands = (*smalls, *weights, *aheads, *matrices)
    return pl.pallas_call(
        kernel,
        out_shape=[
            pltpu.VMEM((count, width), F32),
            pltpu.VMEM((3 * count, devices * MOST), BF16),
            exchange,
            pltpu.VMEM(state.shape, F32),
        ],
        in_specs=[hbm] * len(operands),
        out_specs=[vmem] * 4,
        scratch_shapes=scratch,
        compiler_params=pltpu.CompilerParams(
            collective_id=0, has_side_effects=True, vmem_limit_bytes=VMEM_BYTES
        ),
        name="layer",
    )(*map(pinned, operands))


def close_kernel(kept, weight_pieces, answers, state, out, new_state, mixed, sem, out_sem):
    count = kept.shape[0]
    chunks = sem.shape[0]
    copies = []
    for number in range(chunks):
        span = pl.ds(number * (count // chunks), count // chunks)
        copies.append(pltpu.make_async_copy(state.at[span], new_state.at[span], sem.at[number]))
        copies[-1].start()
    total = weight_pieces.shape[1]
    pieces = dot(weight_pieces[...], answers[...].reshape(total, kept.shape[1]))
    routed = pieces[:count] + pieces[count : 2 * count] + pieces[2 * count :]
    mixed[...] = (kept[...] + routed).astype(BF16)
    copies.append(pltpu.make_async_copy(mixed, out, out_sem))
    copies[-1].start()
    for copy in copies:
        copy.wait()


def close(kept, weight_pieces, answers, state):
    vmem = pl.BlockSpec(memory_space=pltpu.VMEM)
    hbm = pl.BlockSpec(memory_space=pltpu.HBM)
    return pl.pallas_call(
        close_kernel,
        out_shape=[
            jax.ShapeDtypeStruct(kept.shape, BF16),
            jax.ShapeDtypeStruct(state.shape, F32),
        ],
        in_specs=[vmem] * 4,
        out_specs=[hbm, hbm],
        scratch_shapes=[
            pltpu.VMEM(kept.shape, BF16),
            pltpu.SemaphoreType.DMA((8 if state.shape[0] % 8 == 0 else 1,)),
            pltpu.SemaphoreType.DMA,
        ],
        compiler_params=pltpu.CompilerParams(vmem_limit_bytes=CLOSE_BYTES),
        name="close",
    )(kept, weight_pieces, answers, state)


def pinned(array):
    return pltpu.with_memory_space_constraint(array, pltpu.HBM)


def per_device(
    tokens,
    recurrent_state,
    first_gain,
    w_receptance,
    w_key,
    w_value,
    decay_down,
    decay_up,
    decay_base,
    rate_down,
    rate_up,
    rate_base,
    key_scale,
    head_gain,
    w_output,
    second_gain,
    shared_gate,
    shared_up,
    shared_down,
    expert_gate,
    expert_up,
    expert_down,
    routes,
    route_weights,
):
    devices = lax.axis_size("ep")
    results = layer(
        devices,
        (
            tokens,
            first_gain[None, :],
            decay_down.T,
            decay_up,
            decay_base[None, :],
            rate_down.T,
            rate_up,
            rate_base[None, :],
            key_scale[None, :],
        ),
        (w_receptance, w_key, w_value),
        (
            recurrent_state,
            w_output,
            head_gain[None, :],
            second_gain[None, :],
            routes.T,
            route_weights.T,
        ),
        (shared_gate, shared_up, shared_down, expert_gate, expert_up, expert_down),
    )
    return close(*results)


def solution(mesh):
    in_specs = (
        P("ep", None),
        P("ep", None, None),
        P(),
        P("ep", None),
        P("ep", None),
        P("ep", None),
        P(),
        P(),
        P(),
        P(),
        P(),
        P(),
        P(),
        P(),
        P(),
        P(),
        P(),
        P(),
        P(),
        P("ep", None, None),
        P("ep", None, None),
        P("ep", None, None),
        P(),
        P(),
    )
    out_specs = (P("ep", None), P("ep", None, None))
    return jax.shard_map(
        per_device, mesh=mesh, in_specs=in_specs, out_specs=out_specs, check_vma=False
    )
```
